32 devices in a mesh: sp: 16 (over z, y, x), tp: 2 (over core).
Axes of the slice: x: 2, y: 2, z: 4, core: 2. Of those that a mesh axis runs over, the one named last changes fastest.
Arguments:
- queries: bfloat16 [2048, 1024], P('sp', 'tp'), may hold values from -6 to 6
- attn_out: bfloat16 [2048, 1024], P('sp', 'tp'), may hold values from -6 to 6
- out_grad: bfloat16 [2048, 1024], P('sp', 'tp'), may hold values from -384 to 384
- row_lse: float32 [2048, 8], P('sp', 'tp'), may hold values from 9.5 to 12.5
- source: bfloat16 [8192, 4096], P('sp', 'tp'), may hold values from -6 to 6
- saved_keys: bfloat16 [8192, 256], P('sp'), may hold values from -6 to 6
- saved_values: bfloat16 [8192, 256], P('sp'), may hold values from -6 to 6
- key_weight: bfloat16 [4096, 256], P('tp'), may hold values from -0.09375 to 0.09375
- value_weight: bfloat16 [4096, 256], P('tp'), may hold values from -0.09375 to 0.09375
Outputs:
- query_grad: float32 [2048, 1024], P('sp', 'tp')
- source_grad: float32 [8192, 4096], P('sp', 'tp')
- key_grad: float32 [256, 4096], P('sp', 'tp')
The draws below stay inside these ranges and needn't reach their ends.
All inputs are finite; a program needn't handle non-finite values.
Results may differ from the reference program's by a relative error of at most 0.012.
Values may be sent and summed in bfloat16 or wider, within the bound.
A program may use at most 64 MiB of HBM per device.

```python
import math
import jax
import jax.numpy as jnp
from jax import lax

D = 4096
HEADS = 8
KV_HEADS = 2
HEAD_DIM = 128
TARGET_ROWS = 2048
SOURCE_ROWS = 8192


def levels(rng, extent, cuts, smallest, largest):
    def one(position, parts):
        heights = jax.random.uniform(jax.random.fold_in(jax.random.fold_in(rng, 6), position), (parts,), jnp.float32, smallest / len(cuts), largest / len(cuts))
        return jnp.repeat(jnp.exp(heights), extent[position] // parts).reshape((-1,) + (1,) * (len(extent) - position - 1))

    gain = one(*cuts[0])
    for cut in cuts[1:]:
        gain = gain * one(*cut)
    return gain


def normal_values(rng, dims, deviation, reach, pieces=(), dtype=jnp.bfloat16):
    array = deviation * jax.random.normal(rng, dims, jnp.float32)
    if pieces:
        array = array * levels(rng, dims, pieces, -0.22, 0.18)
    return jnp.clip(array, -reach, reach).astype(dtype)


def setup_inputs(seed: int = 0) -> dict:
    arg_keys = jax.random.split(jax.random.key(seed), 10)
    return {
        "queries": normal_values(arg_keys[0], (TARGET_ROWS, HEADS * HEAD_DIM), 1.0, 6.0, ((0, 16), (1, 2))),
        "attn_out": normal_values(arg_keys[1], (TARGET_ROWS, HEADS * HEAD_DIM), 1.0, 6.0, ((0, 16), (1, 2))),
        "out_grad": normal_values(arg_keys[2], (TARGET_ROWS, HEADS * HEAD_DIM), 64.0, 384.0, ((0, 16), (1, 2))),
        "row_lse": jnp.clip(9.5 + 3.0 * jax.random.uniform(arg_keys[3], (TARGET_ROWS, HEADS), jnp.float32) ** levels(arg_keys[3], (TARGET_ROWS, HEADS), ((0, 16), (1, 2)), -0.2, 0.2), 9.5, 12.5),
        "source": normal_values(arg_keys[4], (SOURCE_ROWS, D), 1.0, 6.0, ((0, 16), (1, 2))),
        "saved_keys": normal_values(arg_keys[5], (SOURCE_ROWS, KV_HEADS * HEAD_DIM), 1.0, 6.0, ((0, 16),)),
        "saved_values": normal_values(arg_keys[6], (SOURCE_ROWS, KV_HEADS * HEAD_DIM), 1.0, 6.0, ((0, 16),)),
        "key_weight": normal_values(arg_keys[7], (D, KV_HEADS * HEAD_DIM), D ** -0.5, 0.09375, ((0, 2),)),
        "value_weight": normal_values(arg_keys[8], (D, KV_HEADS * HEAD_DIM), D ** -0.5, 0.09375, ((0, 2),)),
    }


def reference(queries, attn_out, out_grad, row_lse, source, saved_keys, saved_values, key_weight, value_weight):
    per_key = HEADS // KV_HEADS
    score_scale = 1.0 / math.sqrt(HEAD_DIM)
    tgt_len = queries.shape[0]
    src_len = source.shape[0]
    span = math.gcd(tgt_len, 1024)
    count = tgt_len // span
    row_delta = lax.optimization_barrier(jnp.sum((out_grad.astype(jnp.float32) * attn_out.astype(jnp.float32)).reshape(-1, HEADS, HEAD_DIM), axis=2))
    key_acc = jnp.zeros((src_len, KV_HEADS * HEAD_DIM), jnp.float32)
    value_acc = jnp.zeros((src_len, KV_HEADS * HEAD_DIM), jnp.float32)
    head_parts = []
    for head_index in range(HEADS):
        kv_lo = head_index // per_key * HEAD_DIM
        col_lo = head_index * HEAD_DIM
        key_head = saved_keys[:, kv_lo:kv_lo + HEAD_DIM]
        value_head = saved_values[:, kv_lo:kv_lo + HEAD_DIM]
        query_blocks = queries[:, col_lo:col_lo + HEAD_DIM].reshape(count, span, HEAD_DIM)
        grad_blocks = out_grad[:, col_lo:col_lo + HEAD_DIM].reshape(count, span, HEAD_DIM)
        lse_blocks = row_lse[:, head_index:head_index + 1].reshape(count, span, 1)
        delta_blocks = row_delta[:, head_index:head_index + 1].reshape(count, span, 1)

        def step(carry, items):
            key_part, value_part = carry
            query_head, grad_head, lse_col, delta_col = items
            scores = jnp.dot(query_head, key_head.T, preferred_element_type=jnp.float32) * score_scale
            attn_probs = jnp.exp(scores - lse_col)
            dprobs = jnp.dot(grad_head, value_head.T, preferred_element_type=jnp.float32)
            dscores = (attn_probs * (dprobs - delta_col) * score_scale).astype(jnp.bfloat16)
            key_part = key_part + jnp.dot(dscores.T, query_head, preferred_element_type=jnp.float32)
            value_part = value_part + jnp.dot(attn_probs.astype(jnp.bfloat16).T, grad_head, preferred_element_type=jnp.float32)
            return ((key_part, value_part), jnp.dot(dscores, key_head, preferred_element_type=jnp.float32))
        empty = jnp.zeros((src_len, HEAD_DIM), jnp.float32)
        (key_part, value_part), query_blocks_out = lax.scan(step, (empty, empty), (query_blocks, grad_blocks, lse_blocks, delta_blocks))
        head_parts.append(query_blocks_out.reshape(tgt_len, HEAD_DIM))
        key_acc = key_acc.at[:, kv_lo:kv_lo + HEAD_DIM].add(key_part)
        value_acc = value_acc.at[:, kv_lo:kv_lo + HEAD_DIM].add(value_part)
    query_grad = jnp.concatenate(head_parts, axis=1)
    key_half = key_acc.astype(jnp.bfloat16)
    value_half = value_acc.astype(jnp.bfloat16)
    source_grad = jnp.dot(key_half, key_weight.T, preferred_element_type=jnp.float32) + jnp.dot(value_half, value_weight.T, preferred_element_type=jnp.float32)
    key_grad = jnp.dot(key_half.T, source, preferred_element_type=jnp.float32) * (1.0 / math.sqrt(source.shape[0]))
    return (query_grad, source_grad, key_grad)
```

```python
import functools
import math

import jax
import jax.numpy as jnp
from jax import lax
from jax.experimental import pallas as pl
from jax.experimental.pallas import tpu as pltpu
from jax.sharding import PartitionSpec as P

HEADS = 8
KV_HEADS = 2
HEAD_DIM = 128
HALVES = 2
LOG2E = 1.0 / math.log(2.0)
MESH = pl.DeviceIdType.MESH
F32 = jnp.float32
BF16 = jnp.bfloat16
VMEM_BYTES = 67_043_328


def dot_nt(left, right, precision=None):
    return lax.dot_general(
        left, right, (((1,), (1,)), ((), ())), preferred_element_type=F32, precision=precision
    )


def dot_tn(left, right):
    return lax.dot_general(left, right, (((0,), (0,)), ((), ())), preferred_element_type=F32)


def dot_nn(left, right):
    return jnp.dot(left, right, preferred_element_type=F32)


def kernel(
    tgt_n, src_n, key_n, tp_n, src_total,
    q_hbm, o_hbm, d_hbm, lse_hbm, key_hbm, value_hbm, source_hbm, kw_hbm, vw_hbm,
    dq_ref, sg_ref, kg_ref,
    kv_ref, weights,    o_own, lse_own, qd, stats, kvs, dk, dv, dq_acc, dq_out, dq_in, dq_via, g_out, g_in, g_via, tp_own, tp_in,
    src, a_out, a_in, a2_own, a2_out, a2_in, b_out, b_in, b2_own, b2_out, b2_in,
    copy_sem, load_kv, load_q, load_o, qd_s, qd_r, rq_s, st_s, st_r, kv_s, kv_r, rkv_s, dq_s, dq_r, via_r, g_s, g_r, gv_s, gv_r, tp_s, tp_r,
    a_s, a_r, a2_s, a2_r, b_s, b_r, b2_s, b2_r,
):
    sp = lax.axis_index("sp")
    tp = lax.axis_index("tp")
    sp_n = tgt_n * src_n
    t_hi, t_lo = sp // (2 * src_n), sp % 2
    me_t = t_hi * 2 + t_lo
    me_s = (sp // 2) % src_n
    s_hi, s_lo = me_s // 2, me_s % 2
    near_t, near_s = t_hi * 2 + 1 - t_lo, s_hi * 2 + 1 - s_lo
    t_his = [lax.rem(t_hi + k, tgt_n // 2) for k in range(1, tgt_n // 2)]
    s_his = [lax.rem(s_hi + k, src_n // 2) for k in range(1, src_n // 2)]
    far_t = [hi * 2 + t_lo for hi in t_his]
    diag_t = [hi * 2 + 1 - t_lo for hi in t_his]
    far_s = [hi * 2 + s_lo for hi in s_his]
    diag_s = [hi * 2 + 1 - s_lo for hi in s_his]
    t_peers = far_t + [near_t] + diag_t
    s_peers = far_s + [near_s] + diag_s
    key_m = sp_n // key_n
    me_o, me_i = sp // key_n, sp % key_n
    o_peers = [lax.rem(me_o + k, key_m) for k in range(1, key_m)]
    i_peers = [lax.rem(me_i + k, key_n) for k in range(1, key_n)]
    tp_peers = [lax.rem(tp + k, tp_n) for k in range(1, tp_n)]
    rows = q_hbm.shape[0]
    heads = q_hbm.shape[1] // HEAD_DIM
    chunks = stats.shape[1]
    src_rows = dk.shape[1]
    split = (chunks + 1) // 2
    per_chunk = heads // chunks
    per_key = HEADS // KV_HEADS
    scale = 1.0 / math.sqrt(HEAD_DIM)
    kv_col = pl.multiple_of(tp * heads // per_key * HEAD_DIM, HEAD_DIM)

    def t_dev(t):
        return {"sp": t // 2 * (2 * src_n) + me_s * 2 + t % 2, "tp": tp}

    def s_dev(s):
        return {"sp": t_hi * (2 * src_n) + s * 2 + t_lo, "tp": tp}

    def o_dev(o):
        return {"sp": o * key_n + me_i, "tp": tp}

    def i_dev(i):
        return {"sp": me_o * key_n + i, "tp": tp}

    def tp_dev(p):
        return {"sp": sp, "tp": p}

    def remote(source, target, send, recv, device):
        return pltpu.make_async_remote_copy(
            src_ref=source, dst_ref=target, send_sem=send, recv_sem=recv,
            device_id=device, device_id_type=MESH,
        )

    partners = (
        [t_dev(t) for t in t_peers] + [s_dev(s) for s in s_peers]
        + [o_dev(o) for o in o_peers] + [i_dev(i) for i in i_peers] + [tp_dev(p) for p in tp_peers]
    )
    barrier = pltpu.get_barrier_semaphore()
    for device in partners:
        pl.semaphore_signal(barrier, inc=1, device_id=device, device_id_type=MESH)
    piece = src_rows // HALVES
    chunk_w = per_chunk * HEAD_DIM
    loads = []
    for h in range(HALVES):
        for i, ref in enumerate((key_hbm, value_hbm)):
            loads.append(pltpu.make_async_copy(
                ref.at[pl.ds(h * piece, piece), pl.ds(kv_col, HEAD_DIM)],
                kvs.at[me_s, h, i], load_kv.at[2 * h + i],
            ))
    for c in range(chunks):
        for i, ref in enumerate((q_hbm, d_hbm)):
            loads.append(pltpu.make_async_copy(
                ref.at[:, pl.ds(c * chunk_w, chunk_w)], qd.at[me_t, c, i], load_q.at[c, i]
            ))
    loads.append(pltpu.make_async_copy(o_hbm, o_own, load_o.at[0]))
    loads.append(pltpu.make_async_copy(lse_hbm, lse_own, load_o.at[1]))
    lates = [pltpu.make_async_copy(source_hbm, src, copy_sem.at[0])]
    for i, ref in enumerate((kw_hbm, vw_hbm)):
        lates.append(pltpu.make_async_copy(ref, weights.at[i], copy_sem.at[1 + i]))
    for copy in loads:
        copy.start()
    for copy in lates:
        copy.start()
    dk[...] = jnp.zeros_like(dk)
    dv[...] = jnp.zeros_like(dv)
    dq_acc[...] = jnp.zeros_like(dq_acc)
    for copy in loads:
        copy.wait()
    ones = jnp.ones((8, HEAD_DIM), F32)
    for h in range(heads):
        cols = pl.ds(h * HEAD_DIM, HEAD_DIM)
        c, span = h // per_chunk, pl.ds(h % per_chunk * rows, rows)
        grad = qd[me_t, c, 1, :, pl.ds(h % per_chunk * HEAD_DIM, HEAD_DIM)]
        prod = grad.astype(F32) * o_own[:, cols].astype(F32)
        delta = dot_nt(ones, prod, lax.Precision.HIGHEST)
        stats[me_t, c, 0:1, span] = lse_own[h : h + 1, :] * LOG2E
        stats[me_t, c, 1:2, span] = delta[0:1, :]
    pl.semaphore_wait(barrier, len(partners))

    def send_q(t, c):
        return remote(
            qd.at[me_t, c], qd.at[me_t, c], qd_s.at[t, c], qd_r.at[me_t, c], t_dev(t)
        )

    def send_kv(s, h):
        return remote(
            kvs.at[me_s, h], kvs.at[me_s, h], kv_s.at[s, h], kv_r.at[me_s, h], s_dev(s)
        )

    for n in range(max(HALVES, chunks)):
        if n < HALVES:
            for s in far_s + [near_s]:
                send_kv(s, n).start()
        if n < chunks:
            for t in far_t + [near_t]:
                send_q(t, n).start()
        if n == 0:
            for t in t_peers:
                remote(
                    stats.at[me_t], stats.at[me_t], st_s.at[t], st_r.at[me_t], t_dev(t)
                ).start()

    def stack(t, i, c):
        return jnp.concatenate(
            [qd[t, c, i, :, h * HEAD_DIM : (h + 1) * HEAD_DIM] for h in range(per_chunk)], axis=0
        )

    def tile(t, s, low=0, high=chunks):
        def body(c, carry):
            q, d = stack(t, 0, c), stack(t, 1, c)
            k = kvs[s, :, 0].reshape(src_rows, HEAD_DIM)
            v = kvs[s, :, 1].reshape(src_rows, HEAD_DIM)
            scores = dot_nt(k, q)
            probs = jnp.exp2(scores * (scale * LOG2E) - stats[t, c, 0:1, :])
            dprobs = dot_nt(v, d)
            dscores = (probs * (dprobs - stats[t, c, 1:2, :])).astype(BF16)
            dv[s] += dot_nn(probs.astype(BF16), d)
            dk[s] += dot_nn(dscores, q)
            dq_acc[t, c] += dot_tn(dscores, k)
            return carry

        if low < high:
            lax.fori_loop(low, high, body, 0)

    def got_q(t, c):
        remote(qd.at[t, c], qd.at[t, c], qd_s.at[t, c], qd_r.at[t, c], t_dev(t)).wait_recv()

    def got_stats(t):
        remote(stats.at[t], stats.at[t], st_s.at[t], st_r.at[t], t_dev(t)).wait_recv()

    def got_kv(s, h):
        remote(kvs.at[s, h], kvs.at[s, h], kv_s.at[s, h], kv_r.at[s, h], s_dev(s)).wait_recv()

    def relay_q(t, c):
        return remote(
            qd.at[t, c], qd.at[t, c], rq_s.at[t, c], qd_r.at[t, c], t_dev(near_t)
        )

    def relay_kv(s, h):
        return remote(
            kvs.at[s, h], kvs.at[s, h], rkv_s.at[s, h], kv_r.at[s, h], s_dev(near_s)
        )

    def pass_q(low, high):
        for c in range(low, high):
            for t in far_t:
                got_q(t, c)
                relay_q(t, c).start()

    def pass_kv(h):
        for s in far_s:
            got_kv(s, h)
            relay_kv(s, h).start()

    def dq_copy(t):
        return remote(dq_out.at[t], dq_in.at[me_t], dq_s.at[t], dq_r.at[me_t], t_dev(t))

    def g_term(s, i):
        return dv[s] if i else dk[s] * scale

    def g_copy(s, i):
        return remote(
            g_out.at[s, i], g_in.at[me_s, i], g_s.at[s, i], g_r.at[me_s, i], s_dev(s)
        )

    def via_copy(n, i):
        return remote(
            g_out.at[diag_s[n], i], g_via.at[me_s, i], gv_s.at[far_s[n], i],
            gv_r.at[me_s, i], s_dev(far_s[n]),
        )

    def send_via(i):
        for n, s in enumerate(diag_s):
            g_out[s, i] = g_term(s, i).astype(BF16)
            via_copy(n, i).start()

    def send_far(i):
        for s in far_s:
            g_out[s, i] = g_term(s, i).astype(BF16)
            g_copy(s, i).start()

    def send_near(i):
        total = g_term(near_s, i)
        for s in far_s:
            remote(
                g_via.at[s, i], g_via.at[s, i], gv_s.at[s, i], gv_r.at[s, i], s_dev(s)
            ).wait_recv()
            total += g_via[s, i].astype(F32)
        g_out[near_s, i] = total.astype(BF16)
        g_copy(near_s, i).start()

    tile(me_t, me_s)
    got_stats(near_t)
    for c in range(chunks):
        got_q(near_t, c)
        tile(near_t, me_s, c, c + 1)
    pass_kv(0)
    for h in range(HALVES):
        got_kv(near_s, h)
    tile(me_t, near_s)
    pass_q(0, split)
    tile(near_t, near_s)
    for t in far_t:
        got_stats(t)
        for s in [me_s, near_s]:
            tile(t, s, 0, split)
    for h in range(1, HALVES):
        pass_kv(h)
    pass_q(split, chunks)
    for s in far_s:
        for t in [me_t, near_t]:
            tile(t, s)
    for t in far_t:
        for s in [me_s, near_s]:
            tile(t, s, split, chunks)
    for s in diag_s:
        for h in range(HALVES):
            got_kv(s, h)
        for t in [near_t, me_t] + far_t:
            tile(t, s)
    dq_out[near_t] = (dq_acc[near_t] * scale).astype(BF16)
    dq_copy(near_t).start()
    for t in diag_t:
        got_stats(t)
        for c in range(chunks):
            got_q(t, c)
        for s in diag_s:
            tile(t, s)
    send_via(0)
    for s in far_s:
        for t in far_t + diag_t:
            tile(t, s)
    send_far(0)
    for t in diag_t:
        for s in [near_s, me_s]:
            tile(t, s)
    send_near(0)
    for t in diag_t:
        dq_out[t] = (dq_acc[t] * scale).astype(BF16)
        remote(dq_out.at[t], dq_via.at[t], dq_s.at[t], via_r.at[t], t_dev(near_t)).start()
    send_via(1)
    send_far(1)

    def reduce_g(i):
        total = g_term(me_s, i)
        for s in far_s + [near_s]:
            remote(
                g_in.at[s, i], g_in.at[s, i], g_s.at[s, i], g_r.at[s, i], s_dev(s)
            ).wait_recv()
            total += g_in[s, i].astype(F32)
        tp_own[i] = total.astype(BF16)
        for p in tp_peers:
            remote(
                tp_own.at[i], tp_in.at[tp, i], tp_s.at[p, i], tp_r.at[tp, i], tp_dev(p)
            ).start()
        tp_in[tp, i] = tp_own[i]

    def gather_g(i):
        for p in tp_peers:
            remote(
                tp_in.at[p, i], tp_in.at[p, i], tp_s.at[p, i], tp_r.at[p, i], tp_dev(p)
            ).wait_recv()
        for g in range(KV_HEADS):
            owners = [p for p in range(tp_n) if p * heads // per_key == g]
            half = tp_in[owners[0], i]
            if len(owners) > 1:
                total = half.astype(F32)
                for p in owners[1:]:
                    total += tp_in[p, i].astype(F32)
                half = total.astype(BF16)
            kv_ref[:, pl.ds((i * KV_HEADS + g) * HEAD_DIM, HEAD_DIM)] = half

    reduce_g(0)
    lates[0].wait()
    gather_g(0)
    part = a2_own.shape[1]
    cut = a2_own.shape[2]
    key_half = kv_ref[:, 0 : KV_HEADS * HEAD_DIM]
    w_scale = 1.0 / math.sqrt(src_total)
    partial = dot_tn(key_half, src[...]) * w_scale
    for o in range(key_m):
        for i in range(key_n):
            low = (o * key_n + i) * part
            block = partial[low : low + part].astype(BF16)
            a_out[i, o] = block[:, :cut]
            b_out[o, i] = block[:, cut:]
    for i in i_peers:
        remote(a_out.at[i], a_in.at[me_i], a_s.at[i], a_r.at[me_i], i_dev(i)).start()
    for o in o_peers:
        remote(b_out.at[o], b_in.at[me_o], b_s.at[o], b_r.at[me_o], o_dev(o)).start()

    send_near(1)
    for t in far_t:
        remote(dq_out.at[t], dq_via.at[t], dq_s.at[t], via_r.at[t], t_dev(near_t)).wait_recv()
        dq_out[t] = (dq_acc[t] * scale + dq_via[t].astype(F32)).astype(BF16)
        dq_copy(t).start()

    total = b_out[me_o].astype(F32)
    for o in o_peers:
        remote(b_in.at[o], b_in.at[o], b_s.at[o], b_r.at[o], o_dev(o)).wait_recv()
        total += b_in[o].astype(F32)
    b2_own[...] = total
    b2_out[...] = total.astype(BF16)
    for i in i_peers:
        remote(b2_out.at[i], b2_in.at[me_i], b2_s.at[i], b2_r.at[me_i], i_dev(i)).start()
    total = a_out[me_i].astype(F32)
    for i in i_peers:
        remote(a_in.at[i], a_in.at[i], a_s.at[i], a_r.at[i], i_dev(i)).wait_recv()
        total += a_in[i].astype(F32)
    a2_own[...] = total
    a2_out[...] = total.astype(BF16)
    for o in o_peers:
        remote(a2_out.at[o], a2_in.at[me_o], a2_s.at[o], a2_r.at[me_o], o_dev(o)).start()
    reduce_g(1)
    gather_g(1)
    for copy in lates[1:]:
        copy.wait()
    kv_width = KV_HEADS * HEAD_DIM
    span = sg_ref.shape[1] // 4

    def source_tile(n, carry):
        cols = pl.ds(pl.multiple_of(n * span, HEAD_DIM), span)
        sg_ref[:, cols] = dot_nt(kv_ref[:, :kv_width], weights[0, cols, :]) + dot_nt(
            kv_ref[:, kv_width:], weights[1, cols, :]
        )
        return carry

    lax.fori_loop(0, 4, source_tile, 0)
    dq_total = dq_acc[me_t] * scale
    for t in [near_t] + far_t:
        remote(dq_in.at[t], dq_in.at[t], dq_s.at[t], dq_r.at[t], t_dev(t)).wait_recv()
        dq_total += dq_in[t].astype(F32)
    for h in range(heads):
        low = h % per_chunk * rows
        dq_ref[:, h * HEAD_DIM : (h + 1) * HEAD_DIM] = dq_total[h // per_chunk, low : low + rows]

    total = b2_own[me_i]
    for i in i_peers:
        remote(b2_in.at[i], b2_in.at[i], b2_s.at[i], b2_r.at[i], i_dev(i)).wait_recv()
        total += b2_in[i].astype(F32)
    kg_ref[:, cut:] = total
    total = a2_own[me_o]
    for o in o_peers:
        remote(a2_in.at[o], a2_in.at[o], a2_s.at[o], a2_r.at[o], o_dev(o)).wait_recv()
        total += a2_in[o].astype(F32)
    kg_ref[:, :cut] = total

    for c in range(chunks):
        for t in far_t + [near_t]:
            send_q(t, c).wait_send()
        for t in far_t:
            relay_q(t, c).wait_send()
    for h in range(HALVES):
        for s in far_s + [near_s]:
            send_kv(s, h).wait_send()
        for s in far_s:
            relay_kv(s, h).wait_send()
    for t in t_peers:
        remote(stats.at[t], stats.at[t], st_s.at[t], st_r.at[t], t_dev(t)).wait_send()
        remote(dq_out.at[t], dq_in.at[t], dq_s.at[t], dq_r.at[t], t_dev(t)).wait_send()
    for i in range(2):
        for s in far_s + [near_s]:
            g_copy(s, i).wait_send()
        for n in range(len(diag_s)):
            via_copy(n, i).wait_send()
    for i in i_peers:
        remote(a_out.at[i], a_in.at[i], a_s.at[i], a_r.at[i], i_dev(i)).wait_send()
        remote(b2_out.at[i], b2_in.at[i], b2_s.at[i], b2_r.at[i], i_dev(i)).wait_send()
    for o in o_peers:
        remote(b_out.at[o], b_in.at[o], b_s.at[o], b_r.at[o], o_dev(o)).wait_send()
        remote(a2_out.at[o], a2_in.at[o], a2_s.at[o], a2_r.at[o], o_dev(o)).wait_send()
    for p in tp_peers:
        for i in range(2):
            remote(
                tp_own.at[i], tp_in.at[p, i], tp_s.at[p, i], tp_r.at[p, i], tp_dev(p)
            ).wait_send()


def finish(*refs):
    *refs, sem = refs
    copies = [
        pltpu.make_async_copy(value, out, sem.at[n])
        for n, (value, out) in enumerate(zip(refs[:3], refs[3:]))
    ]
    for copy in copies:
        copy.start()
    for copy in copies:
        copy.wait()


def shards(
    tgt_n, src_n, tp_n,
    queries, attn_out, out_grad, row_lse, source, saved_keys, saved_values, key_weight, value_weight
):
    heads = row_lse.shape[1]
    rows, width = queries.shape
    src_rows, columns = source.shape
    kv_width = KV_HEADS * HEAD_DIM
    sp_n = tgt_n * src_n
    part = kv_width // sp_n
    key_n, key_m = src_n, tgt_n
    chunks = math.gcd(heads, 2)
    stacked = heads // chunks * rows
    cut = (2 * columns // 3 + 127) // 128 * 128
    rest = columns - cut
    dma = pltpu.SemaphoreType.DMA
    vmem = pl.BlockSpec(memory_space=pltpu.VMEM)
    hbm = pl.BlockSpec(memory_space=pltpu.HBM)
    scratch = [
        pltpu.VMEM((src_rows, 2 * kv_width), BF16),
        pltpu.VMEM((2, columns, kv_width), BF16),
        pltpu.VMEM((rows, width), BF16),
        pltpu.VMEM((heads, rows), F32),
        pltpu.VMEM((tgt_n, chunks, 2, rows, width // chunks), BF16),
        pltpu.VMEM((tgt_n, chunks, 8, stacked), F32),
        pltpu.VMEM((src_n, HALVES, 2, src_rows // HALVES, HEAD_DIM), BF16),
        pltpu.VMEM((src_n, src_rows, HEAD_DIM), F32),
        pltpu.VMEM((src_n, src_rows, HEAD_DIM), F32),
        pltpu.VMEM((tgt_n, chunks, stacked, HEAD_DIM), F32),
        pltpu.VMEM((tgt_n, chunks, stacked, HEAD_DIM), BF16),
        pltpu.VMEM((tgt_n, chunks, stacked, HEAD_DIM), BF16),
        pltpu.VMEM((tgt_n, chunks, stacked, HEAD_DIM), BF16),
        pltpu.VMEM((src_n, 2, src_rows, HEAD_DIM), BF16),
        pltpu.VMEM((src_n, 2, src_rows, HEAD_DIM), BF16),
        pltpu.VMEM((src_n, 2, src_rows, HEAD_DIM), BF16),
        pltpu.VMEM((2, src_rows, HEAD_DIM), BF16),
        pltpu.VMEM((tp_n, 2, src_rows, HEAD_DIM), BF16),
        pltpu.VMEM((src_rows, columns), BF16),
        pltpu.VMEM((key_n, key_m, part, cut), BF16),
        pltpu.VMEM((key_n, key_m, part, cut), BF16),
        pltpu.VMEM((key_m, part, cut), F32),
        pltpu.VMEM((key_m, part, cut), BF16),
        pltpu.VMEM((key_m, part, cut), BF16),
        pltpu.VMEM((key_m, key_n, part, rest), BF16),
        pltpu.VMEM((key_m, key_n, part, rest), BF16),
        pltpu.VMEM((key_n, part, rest), F32),
        pltpu.VMEM((key_n, part, rest), BF16),
        pltpu.VMEM((key_n, part, rest), BF16),
        dma((3,)),
        dma((2 * HALVES,)),
        dma((chunks, 2)),
        dma((2,)),
    ]
    for shape in (
        (tgt_n, chunks), (tgt_n, chunks), (tgt_n, chunks), (tgt_n,), (tgt_n,),
        (src_n, HALVES), (src_n, HALVES), (src_n, HALVES), (tgt_n,), (tgt_n,), (tgt_n,),
        (src_n, 2), (src_n, 2), (src_n, 2), (src_n, 2),
        (tp_n, 2), (tp_n, 2), (key_n,), (key_n,), (key_m,), (key_m,),
        (key_m,), (key_m,), (key_n,), (key_n,),
    ):
        scratch.append(dma(shape))
    shapes = ((rows, width), (src_rows, columns), (part, columns))
    grads = pl.pallas_call(
        functools.partial(kernel, tgt_n, src_n, key_n, tp_n, src_rows * sp_n),
        out_shape=[pltpu.VMEM(shape, F32) for shape in shapes],
        in_specs=[hbm] * 9,
        out_specs=[vmem] * 3,
        scratch_shapes=scratch,
        compiler_params=pltpu.CompilerParams(
            collective_id=0, has_side_effects=True,
            vmem_limit_bytes=VMEM_BYTES - 4 * sum(map(math.prod, shapes)),
        ),
        name="attention_grads",
    )(
        queries, attn_out, out_grad, row_lse.T, saved_keys, saved_values, source,
        key_weight, value_weight,
    )
    return tuple(pl.pallas_call(
        finish,
        out_shape=[jax.ShapeDtypeStruct(shape, F32) for shape in shapes],
        in_specs=[vmem] * 3,
        out_specs=[hbm] * 3,
        scratch_shapes=[dma((3,))],
        compiler_params=pltpu.CompilerParams(vmem_limit_bytes=2**20),
        name="write_grads",
    )(*grads))


def solution(mesh):
    sp_n, tp_n = mesh.shape["sp"], mesh.shape["tp"]
    src_n = 2 ** (int(math.log2(sp_n)) // 2)
    in_specs = (
        P("sp", "tp"),
        P("sp", "tp"),
        P("sp", "tp"),
        P("sp", "tp"),
        P("sp", "tp"),
        P("sp", None),
        P("sp", None),
        P("tp", None),
        P("tp", None),
    )
    out_specs = (P("sp", "tp"), P("sp", "tp"), P("sp", "tp"))
    return jax.shard_map(
        functools.partial(shards, sp_n // src_n, src_n, tp_n),
        mesh=mesh, in_specs=in_specs, out_specs=out_specs, check_vma=False,
    )
```

```python
import functools
import math

import jax
import jax.numpy as jnp
from jax import lax
from jax.experimental import pallas as pl
from jax.experimental.pallas import tpu as pltpu
from jax.sharding import PartitionSpec as P

HEADS = 8
KV_HEADS = 2
HEAD_DIM = 128
HALVES = 2
PIECES = 3
LOG2E = 1.0 / math.log(2.0)
MESH = pl.DeviceIdType.MESH
F32 = jnp.float32
BF16 = jnp.bfloat16
VMEM_BYTES = 67_043_328


def dot_nt(left, right, precision=None):
    return lax.dot_general(
        left, right, (((1,), (1,)), ((), ())), preferred_element_type=F32, precision=precision
    )


def dot_tn(left, right):
    return lax.dot_general(left, right, (((0,), (0,)), ((), ())), preferred_element_type=F32)


def dot_nn(left, right):
    return jnp.dot(left, right, preferred_element_type=F32)


def kernel(
    tgt_n, src_n, key_n, tp_n, src_total,
    q_hbm, o_hbm, d_hbm, lse_hbm, key_hbm, value_hbm, source_hbm, kw_hbm, vw_hbm,
    dq_ref, sg_ref, kg_ref,
    kv_ref, weights,    o_own, lse_own, qd, stats, kvs, dk, dv, dq_acc, dq_out, dq_in, d_out, g_via, g_out, g_in, tp_own, tp_in,
    src, a_out, a_in, a2_own, a2_out, a2_in, b_out, b_in, b2_own, b2_out, b2_in,
    copy_sem, load_kv, load_q, load_o, up_s, down_s, qd_r, st_s, st_r, kvx_s, kvy_s, kv_r, rkv_s, dq_s, dq_r, via_s, via_r, g_s, g_r, tp_s, tp_r,
    a_s, a_r, a2_s, a2_r, b_s, b_r, b2_s, b2_r,
):
    sp = lax.axis_index("sp")
    tp = lax.axis_index("tp")
    sp_n = tgt_n * src_n
    me_t, me_s = sp // src_n, sp % src_n
    x_s = me_s + 1 - 2 * (me_s % 2)
    y_s, d_s = (me_s + 2) % src_n, (x_s + 2) % src_n
    s_peers = [d_s, x_s, y_s]
    t_peers = [lax.rem(me_t + k, tgt_n) for k in range(1, tgt_n)]
    below, above = me_t, tgt_n - 1 - me_t
    paired = jnp.minimum(below, above)
    longer = jnp.where(above > below, 1, -1)
    inner = paired > 0
    order = []
    for j in range(tgt_n - 1):
        both = me_t + (j // 2 + 1) * (1 if j % 2 == 0 else -1)
        order.append(jnp.where(j < 2 * paired, both, me_t + longer * (j - paired + 1)))
    key_m = tgt_n
    me_o, me_i = me_t, me_s
    o_peers, i_peers = t_peers, s_peers
    tp_peers = [lax.rem(tp + k, tp_n) for k in range(1, tp_n)]
    rows = q_hbm.shape[0]
    heads = q_hbm.shape[1] // HEAD_DIM
    chunks = qd.shape[1]
    src_rows = dk.shape[1]
    stacked = stats.shape[2]
    split = (chunks + 1) // 2
    per_chunk = heads // chunks
    per_key = HEADS // KV_HEADS
    scale = 1.0 / math.sqrt(HEAD_DIM)
    kv_col = pl.multiple_of(tp * heads // per_key * HEAD_DIM, HEAD_DIM)

    def t_dev(t):
        return {"sp": t * src_n + me_s, "tp": tp}

    def s_dev(s):
        return {"sp": me_t * src_n + s, "tp": tp}

    o_dev, i_dev = t_dev, s_dev

    def tp_dev(p):
        return {"sp": sp, "tp": p}

    def remote(source, target, send, recv, device):
        return pltpu.make_async_remote_copy(
            src_ref=source, dst_ref=target, send_sem=send, recv_sem=recv,
            device_id=device, device_id_type=MESH,
        )

    partners = (
        [t_dev(t) for t in t_peers] + [s_dev(s) for s in s_peers] + [tp_dev(p) for p in tp_peers]
    )
    barrier = pltpu.get_barrier_semaphore()
    for device in partners:
        pl.semaphore_signal(barrier, inc=1, device_id=device, device_id_type=MESH)
    piece = src_rows // HALVES
    chunk_w = per_chunk * HEAD_DIM
    loads = []
    for h in range(HALVES):
        for i, ref in enumerate((key_hbm, value_hbm)):
            loads.append(pltpu.make_async_copy(
                ref.at[pl.ds(h * piece, piece), pl.ds(kv_col, HEAD_DIM)],
                kvs.at[me_s, h, i], load_kv.at[2 * h + i],
            ))
    for c in range(chunks):
        for i, ref in enumerate((q_hbm, d_hbm)):
            loads.append(pltpu.make_async_copy(
                ref.at[:, pl.ds(c * chunk_w, chunk_w)], qd.at[me_t, c, i], load_q.at[c, i]
            ))
    loads.append(pltpu.make_async_copy(o_hbm, o_own, load_o.at[0]))
    loads.append(pltpu.make_async_copy(lse_hbm, lse_own, load_o.at[1]))
    lates = [pltpu.make_async_copy(source_hbm, src, copy_sem.at[0])]
    for i, ref in enumerate((kw_hbm, vw_hbm)):
        lates.append(pltpu.make_async_copy(ref, weights.at[i], copy_sem.at[1 + i]))
    for copy in loads:
        copy.start()
    dk[...] = jnp.zeros_like(dk)
    dv[...] = jnp.zeros_like(dv)
    dq_acc[...] = jnp.zeros_like(dq_acc)
    for copy in loads:
        copy.wait()
    ones = jnp.ones((8, HEAD_DIM), F32)
    for h in range(heads):
        cols = pl.ds(h * HEAD_DIM, HEAD_DIM)
        c, span = h // per_chunk, pl.ds(h % per_chunk * rows, rows)
        grad = qd[me_t, c, 1, :, pl.ds(h % per_chunk * HEAD_DIM, HEAD_DIM)]
        prod = grad.astype(F32) * o_own[:, cols].astype(F32)
        delta = dot_nt(ones, prod, lax.Precision.HIGHEST)
        stats[me_t, 2 * c : 2 * c + 1, span] = lse_own[h : h + 1, :] * LOG2E
        stats[me_t, 2 * c + 1 : 2 * c + 2, span] = delta[0:1, :]
    pl.semaphore_wait(barrier, len(partners))
    for copy in lates:
        copy.start()

    def q_copy(block, t, c, sems):
        return remote(
            qd.at[block, c], qd.at[block, c], sems.at[block, c], qd_r.at[block, c], t_dev(t)
        )

    def kv_copy(block, s, h, sems):
        return remote(
            kvs.at[block, h], kvs.at[block, h], sems.at[h], kv_r.at[block, h], s_dev(s)
        )

    def stat_copy(t):
        return remote(stats.at[me_t], stats.at[me_t], st_s.at[t], st_r.at[me_t], t_dev(t))

    def on_line(act):
        @pl.when(above > 0)
        def _():
            act(me_t + 1, up_s)

        @pl.when(below > 0)
        def _():
            act(me_t - 1, down_s)

    for n in range(max(HALVES, chunks)):
        if n < HALVES:
            kv_copy(me_s, x_s, HALVES - 1 - n, kvx_s).start()
            kv_copy(me_s, y_s, n, kvy_s).start()
        if n < chunks:
            on_line(lambda t, sems, n=n: q_copy(me_t, t, n, sems).start())
        if n == 0:
            for t in t_peers:
                stat_copy(t).start()

    def stack(t, i, low, high):
        return jnp.concatenate(
            [
                qd[t, c, i, :, h * HEAD_DIM : (h + 1) * HEAD_DIM]
                for c in range(low, high) for h in range(per_chunk)
            ],
            axis=0,
        )

    def stat(t, i, low, high):
        return jnp.concatenate([stats[t, 2 * c + i : 2 * c + i + 1, :] for c in range(low, high)], axis=1)

    def keys(s, i):
        return kvs[s, :, i].reshape(src_rows, HEAD_DIM)

    def tile(t, s, low=0, high=chunks):
        if low == high:
            return
        q, d = stack(t, 0, low, high), stack(t, 1, low, high)
        k, v = keys(s, 0), keys(s, 1)
        scores = dot_nt(k, q)
        probs = jnp.exp2(scores * (scale * LOG2E) - stat(t, 0, low, high))
        dprobs = dot_nt(v, d)
        dscores = (probs * (dprobs - stat(t, 1, low, high))).astype(BF16)
        probs = probs.astype(BF16)
        dv[s] += dot_nn(probs, d)
        dk[s] += dot_nn(dscores, q)
        part_q = dot_tn(k, dscores)
        for c in range(low, high):
            span = (c - low) * stacked
            dq_acc[t, c] += part_q[:, span : span + stacked]

    def got_q(j, c):
        q_copy(order[j], me_t, c, up_s).wait_recv()

    def forward(j, c, act):
        @pl.when(order[j] > me_t)
        def _():
            act(q_copy(order[j], me_t - 1, c, down_s))

        @pl.when(order[j] < me_t)
        def _():
            act(q_copy(order[j], me_t + 1, c, up_s))

    def pass_q(j, c):
        @pl.when(inner)
        def _():
            got_q(j, c)
            forward(j, c, lambda copy: copy.start())

    def last_q(j, c):
        @pl.when(jnp.logical_not(inner))
        def _():
            got_q(j, c)

    def got_stats(t):
        remote(stats.at[t], stats.at[t], st_s.at[t], st_r.at[t], t_dev(t)).wait_recv()

    def got_kv(s, h):
        kv_copy(s, s, h, kvx_s).wait_recv()

    def dq_copy(t):
        return remote(dq_out.at[t], dq_in.at[me_t], dq_s.at[t], dq_r.at[me_t], t_dev(t))

    def g_part(s, i, h):
        span = pl.ds(h * piece, piece)
        return dv[s, span] if i else dk[s, span] * scale

    def via_copy(i, h):
        return remote(
            d_out.at[i, h], g_via.at[i, h], via_s.at[i, h], via_r.at[i, h], s_dev((x_s, y_s)[h])
        )

    def g_copy(i, n, h):
        return remote(
            g_out.at[i, n, h], g_in.at[i, n, h], g_s.at[i, n, h], g_r.at[i, n, h],
            s_dev((x_s, y_s)[n]),
        )

    def send_via(i):
        for h in range(HALVES):
            d_out[i, h] = g_part(d_s, i, h).astype(BF16)
            via_copy(i, h).start()

    def send_plain(i, n):
        g_out[i, n, n] = g_part((x_s, y_s)[n], i, n).astype(BF16)
        g_copy(i, n, n).start()

    def send_sum(i):
        for h in range(HALVES):
            n = 1 - h
            via_copy(i, h).wait_recv()
            total = g_part((x_s, y_s)[n], i, h) + g_via[i, h].astype(F32)
            g_out[i, n, h] = total.astype(BF16)
            g_copy(i, n, h).start()

    def send_dq(t):
        dq_out[t] = (dq_acc[t] * scale).astype(BF16)
        dq_copy(t).start()

    everyone = [me_s, x_s, y_s, d_s]
    tile(me_t, me_s)
    got_kv(y_s, 0)
    kv_copy(y_s, x_s, 0, rkv_s).start()
    for h in range(1, HALVES):
        got_kv(x_s, h)
        kv_copy(x_s, y_s, h, rkv_s).start()
    for c in range(split):
        pass_q(0, c)
        last_q(0, c)
        pass_q(1, c)
    got_stats(order[0])
    tile(order[0], me_s, 0, split)
    for h in range(1, HALVES):
        got_kv(y_s, h)
    got_kv(x_s, 0)
    for c in range(split, chunks):
        pass_q(0, c)
        last_q(0, c)
        pass_q(1, c)
    tile(order[0], me_s, split, chunks)
    for s in (x_s, y_s):
        tile(me_t, s)
    tile(order[0], x_s)
    for c in range(split):
        pass_q(2, c)
    for h in range(HALVES):
        got_kv(d_s, h)
    tile(order[0], y_s)
    for t in (me_t, order[0]):
        tile(t, d_s)
    send_dq(order[0])
    for c in range(split, chunks):
        pass_q(2, c)
    got_stats(order[1])
    for c in range(chunks):
        last_q(1, c)
    for s in everyone:
        tile(order[1], s)
    send_dq(order[1])
    for j in range(2, tgt_n - 1):
        got_stats(order[j])
        for c in range(chunks):
            if j > 2:
                pass_q(j, c)
            last_q(j, c)
            if c == split - 1:
                for s in everyone:
                    tile(order[j], s, 0, split)
        if j < tgt_n - 2:
            for s in everyone:
                tile(order[j], s, split, chunks)
            send_dq(order[j])
    for n, s in enumerate([d_s, x_s, y_s, me_s]):
        tile(order[-1], s, split, chunks)
        if n == 0:
            send_via(0)
        elif n < 3:
            send_plain(0, n - 1)
    send_dq(order[-1])
    send_sum(0)
    send_via(1)
    for n in range(2):
        send_plain(1, n)

    def reduce_g(i):
        for h in range(HALVES):
            total = g_part(me_s, i, h)
            for n in range(2):
                g_copy(i, n, h).wait_recv()
                total += g_in[i, n, h].astype(F32)
            tp_own[i, h * piece : (h + 1) * piece] = total.astype(BF16)
        for p in tp_peers:
            remote(
                tp_own.at[i], tp_in.at[tp, i], tp_s.at[p, i], tp_r.at[tp, i], tp_dev(p)
            ).start()
        tp_in[tp, i] = tp_own[i]

    def gather_g(i):
        for p in tp_peers:
            remote(
                tp_in.at[p, i], tp_in.at[p, i], tp_s.at[p, i], tp_r.at[p, i], tp_dev(p)
            ).wait_recv()
        for g in range(KV_HEADS):
            owners = [p for p in range(tp_n) if p * heads // per_key == g]
            half = tp_in[owners[0], i]
            if len(owners) > 1:
                total = half.astype(F32)
                for p in owners[1:]:
                    total += tp_in[p, i].astype(F32)
                half = total.astype(BF16)
            kv_ref[:, pl.ds((i * KV_HEADS + g) * HEAD_DIM, HEAD_DIM)] = half

    reduce_g(0)
    lates[0].wait()
    gather_g(0)
    pieces, part, cut = a2_own.shape[0], a2_own.shape[2], a2_own.shape[3]
    key_half = kv_ref[:, 0 : KV_HEADS * HEAD_DIM]
    w_scale = 1.0 / math.sqrt(src_total)

    def a_copy(p, i):
        return remote(
            a_out.at[p, i], a_in.at[p, me_i], a_s.at[p, i], a_r.at[p, me_i], i_dev(i)
        )

    def a2_copy(p, o):
        return remote(
            a2_out.at[p, o], a2_in.at[p, me_o], a2_s.at[p, o], a2_r.at[p, me_o], o_dev(o)
        )

    def a_part(p):
        partial = dot_tn(key_half, src[:, p * cut : (p + 1) * cut]) * w_scale
        for o in range(key_m):
            for i in range(key_n):
                low = (o * key_n + i) * part
                a_out[p, i, o] = partial[low : low + part].astype(BF16)
        for i in i_peers:
            a_copy(p, i).start()

    a_part(0)
    partial = dot_tn(key_half, src[:, pieces * cut :]) * w_scale
    for o in range(key_m):
        for i in range(key_n):
            low = (o * key_n + i) * part
            b_out[o, i] = partial[low : low + part].astype(BF16)
    for o in o_peers:
        remote(b_out.at[o], b_in.at[me_o], b_s.at[o], b_r.at[me_o], o_dev(o)).start()
    for p in range(1, pieces):
        a_part(p)
    send_sum(1)

    def a_sum(p):
        total = a_out[p, me_i].astype(F32)
        for i in i_peers:
            remote(
                a_in.at[p, i], a_in.at[p, i], a_s.at[p, i], a_r.at[p, i], i_dev(i)
            ).wait_recv()
            total += a_in[p, i].astype(F32)
        a2_own[p] = total
        a2_out[p] = total.astype(BF16)
        for o in o_peers:
            a2_copy(p, o).start()

    a_sum(0)
    total = b_out[me_o].astype(F32)
    for o in o_peers:
        remote(b_in.at[o], b_in.at[o], b_s.at[o], b_r.at[o], o_dev(o)).wait_recv()
        total += b_in[o].astype(F32)
    b2_own[...] = total
    b2_out[...] = total.astype(BF16)
    for i in i_peers:
        remote(b2_out.at[i], b2_in.at[me_i], b2_s.at[i], b2_r.at[me_i], i_dev(i)).start()
    for p in range(1, pieces):
        a_sum(p)

    reduce_g(1)
    gather_g(1)
    for copy in lates[1:]:
        copy.wait()
    kv_width = KV_HEADS * HEAD_DIM
    span = sg_ref.shape[1] // 4

    def source_tile(n, carry):
        cols = pl.ds(pl.multiple_of(n * span, HEAD_DIM), span)
        sg_ref[:, cols] = dot_nt(kv_ref[:, :kv_width], weights[0, cols, :]) + dot_nt(
            kv_ref[:, kv_width:], weights[1, cols, :]
        )
        return carry

    lax.fori_loop(0, 4, source_tile, 0)
    dq_total = dq_acc[me_t] * scale
    for t in t_peers:
        remote(dq_in.at[t], dq_in.at[t], dq_s.at[t], dq_r.at[t], t_dev(t)).wait_recv()
        dq_total += dq_in[t].astype(F32)
    for h in range(heads):
        low = h % per_chunk * rows
        block = dq_total[h // per_chunk, :, low : low + rows]
        dq_ref[:, h * HEAD_DIM : (h + 1) * HEAD_DIM] = block.T

    for c in range(chunks):
        on_line(lambda t, sems, c=c: q_copy(me_t, t, c, sems).wait_send())
        for j in range(tgt_n - 1):
            @pl.when(inner)
            def _(j=j, c=c):
                forward(j, c, lambda copy: copy.wait_send())
    for t in t_peers:
        stat_copy(t).wait_send()
        dq_copy(t).wait_send()
    for h in range(HALVES):
        kv_copy(me_s, x_s, h, kvx_s).wait_send()
        kv_copy(me_s, y_s, h, kvy_s).wait_send()
        relayed = (y_s, x_s) if h == 0 else (x_s, y_s)
        kv_copy(*relayed, h, rkv_s).wait_send()
    for i in range(2):
        for h in range(HALVES):
            via_copy(i, h).wait_send()
            for n in range(2):
                g_copy(i, n, h).wait_send()
    for i in i_peers:
        for p in range(pieces):
            a_copy(p, i).wait_send()
        remote(b2_out.at[i], b2_in.at[i], b2_s.at[i], b2_r.at[i], i_dev(i)).wait_send()
    for o in o_peers:
        remote(b_out.at[o], b_in.at[o], b_s.at[o], b_r.at[o], o_dev(o)).wait_send()
        for p in range(pieces):
            a2_copy(p, o).wait_send()
    for p in tp_peers:
        for i in range(2):
            remote(
                tp_own.at[i], tp_in.at[p, i], tp_s.at[p, i], tp_r.at[p, i], tp_dev(p)
            ).wait_send()

    total = b2_own[me_i]
    for i in i_peers:
        remote(b2_in.at[i], b2_in.at[i], b2_s.at[i], b2_r.at[i], i_dev(i)).wait_recv()
        total += b2_in[i].astype(F32)
    kg_ref[:, pieces * cut :] = total
    for p in range(pieces):
        total = a2_own[p, me_o]
        for o in o_peers:
            remote(
                a2_in.at[p, o], a2_in.at[p, o], a2_s.at[p, o], a2_r.at[p, o], o_dev(o)
            ).wait_recv()
            total += a2_in[p, o].astype(F32)
        kg_ref[:, p * cut : (p + 1) * cut] = total


def finish(*refs):
    *refs, sem = refs
    copies = [
        pltpu.make_async_copy(value, out, sem.at[n])
        for n, (value, out) in enumerate(zip(refs[:3], refs[3:]))
    ]
    for copy in copies:
        copy.start()
    for copy in copies:
        copy.wait()


def shards(
    tgt_n, src_n, tp_n,
    queries, attn_out, out_grad, row_lse, source, saved_keys, saved_values, key_weight, value_weight
):
    heads = row_lse.shape[1]
    rows, width = queries.shape
    src_rows, columns = source.shape
    kv_width = KV_HEADS * HEAD_DIM
    sp_n = tgt_n * src_n
    part = kv_width // sp_n
    key_n, key_m = src_n, tgt_n
    chunks = math.gcd(heads, 2)
    stacked = heads // chunks * rows
    cut = columns // (PIECES + 1) // HEAD_DIM * HEAD_DIM
    rest = columns - PIECES * cut
    dma = pltpu.SemaphoreType.DMA
    vmem = pl.BlockSpec(memory_space=pltpu.VMEM)
    hbm = pl.BlockSpec(memory_space=pltpu.HBM)
    scratch = [
        pltpu.VMEM((src_rows, 2 * kv_width), BF16),
        pltpu.VMEM((2, columns, kv_width), BF16),
        pltpu.VMEM((rows, width), BF16),
        pltpu.VMEM((heads, rows), F32),
        pltpu.VMEM((tgt_n, chunks, 2, rows, width // chunks), BF16),
        pltpu.VMEM((tgt_n, 8, stacked), F32),
        pltpu.VMEM((src_n, HALVES, 2, src_rows // HALVES, HEAD_DIM), BF16),
        pltpu.VMEM((src_n, src_rows, HEAD_DIM), F32),
        pltpu.VMEM((src_n, src_rows, HEAD_DIM), F32),
        pltpu.VMEM((tgt_n, chunks, HEAD_DIM, stacked), F32),
        pltpu.VMEM((tgt_n, chunks, HEAD_DIM, stacked), BF16),
        pltpu.VMEM((tgt_n, chunks, HEAD_DIM, stacked), BF16),
        pltpu.VMEM((2, HALVES, src_rows // HALVES, HEAD_DIM), BF16),
        pltpu.VMEM((2, HALVES, src_rows // HALVES, HEAD_DIM), BF16),
        pltpu.VMEM((2, 2, HALVES, src_rows // HALVES, HEAD_DIM), BF16),
        pltpu.VMEM((2, 2, HALVES, src_rows // HALVES, HEAD_DIM), BF16),
        pltpu.VMEM((2, src_rows, HEAD_DIM), BF16),
        pltpu.VMEM((tp_n, 2, src_rows, HEAD_DIM), BF16),
        pltpu.VMEM((src_rows, columns), BF16),
        pltpu.VMEM((PIECES, key_n, key_m, part, cut), BF16),
        pltpu.VMEM((PIECES, key_n, key_m, part, cut), BF16),
        pltpu.VMEM((PIECES, key_m, part, cut), F32),
        pltpu.VMEM((PIECES, key_m, part, cut), BF16),
        pltpu.VMEM((PIECES, key_m, part, cut), BF16),
        pltpu.VMEM((key_m, key_n, part, rest), BF16),
        pltpu.VMEM((key_m, key_n, part, rest), BF16),
        pltpu.VMEM((key_n, part, rest), F32),
        pltpu.VMEM((key_n, part, rest), BF16),
        pltpu.VMEM((key_n, part, rest), BF16),
        dma((3,)),
        dma((2 * HALVES,)),
        dma((chunks, 2)),
        dma((2,)),
    ]
    for shape in (
        (tgt_n, chunks), (tgt_n, chunks), (tgt_n, chunks), (tgt_n,), (tgt_n,),
        (HALVES,), (HALVES,), (src_n, HALVES), (HALVES,), (tgt_n,), (tgt_n,),
        (2, HALVES), (2, HALVES), (2, 2, HALVES), (2, 2, HALVES),
        (tp_n, 2), (tp_n, 2), (PIECES, key_n), (PIECES, key_n), (PIECES, key_m), (PIECES, key_m),
        (key_m,), (key_m,), (key_n,), (key_n,),
    ):
        scratch.append(dma(shape))
    shapes = ((rows, width), (src_rows, columns), (part, columns))
    grads = pl.pallas_call(
        functools.partial(kernel, tgt_n, src_n, key_n, tp_n, src_rows * sp_n),
        out_shape=[pltpu.VMEM(shape, F32) for shape in shapes],
        in_specs=[hbm] * 9,
        out_specs=[vmem] * 3,
        scratch_shapes=scratch,
        compiler_params=pltpu.CompilerParams(
            collective_id=0, has_side_effects=True,
            vmem_limit_bytes=VMEM_BYTES - 4 * sum(map(math.prod, shapes)),
        ),
        name="attention_grads",
    )(
        queries, attn_out, out_grad, row_lse.T, saved_keys, saved_values, source,
        key_weight, value_weight,
    )
    return tuple(pl.pallas_call(
        finish,
        out_shape=[jax.ShapeDtypeStruct(shape, F32) for shape in shapes],
        in_specs=[vmem] * 3,
        out_specs=[hbm] * 3,
        scratch_shapes=[dma((3,))],
        compiler_params=pltpu.CompilerParams(vmem_limit_bytes=2**20),
        name="write_grads",
    )(*grads))


def solution(mesh):
    sp_n, tp_n = mesh.shape["sp"], mesh.shape["tp"]
    src_n = math.gcd(sp_n, 4)
    in_specs = (
        P("sp", "tp"),
        P("sp", "tp"),
        P("sp", "tp"),
        P("sp", "tp"),
        P("sp", "tp"),
        P("sp", None),
        P("sp", None),
        P("tp", None),
        P("tp", None),
    )
    out_specs = (P("sp", "tp"), P("sp", "tp"), P("sp", "tp"))
    return jax.shard_map(
        functools.partial(shards, sp_n // src_n, src_n, tp_n),
        mesh=mesh, in_specs=in_specs, out_specs=out_specs, check_vma=False,
    )
```

```python
import functools
import math

import jax
import jax.numpy as jnp
from jax import lax
from jax.experimental import pallas as pl
from jax.experimental.pallas import tpu as pltpu
from jax.sharding import PartitionSpec as P

HEADS = 8
KV_HEADS = 2
HEAD_DIM = 128
HALVES = 2
PIECES = 3
LOG2E = 1.0 / math.log(2.0)
MESH = pl.DeviceIdType.MESH
F32 = jnp.float32
BF16 = jnp.bfloat16
VMEM_BYTES = 67_043_328


def dot_nt(left, right, precision=None):
    return lax.dot_general(
        left, right, (((1,), (1,)), ((), ())), preferred_element_type=F32, precision=precision
    )


def dot_tn(left, right):
    return lax.dot_general(left, right, (((0,), (0,)), ((), ())), preferred_element_type=F32)


def dot_nn(left, right):
    return jnp.dot(left, right, preferred_element_type=F32)


def kernel(
    tgt_n, src_n, key_n, tp_n, src_total,
    q_hbm, o_hbm, d_hbm, lse_hbm, key_hbm, value_hbm, source_hbm, kw_hbm, vw_hbm,
    dq_ref, sg_ref, kg_ref,
    kv_ref, weights,    o_own, lse_own, qd, stats, kvs, dk, dv, dq_acc, dq_out, dq_in, d_out, g_via, g_out, g_in, tp_own, tp_in,
    src, a_out, a_in, a2_own, a2_out, a2_in, b_out, b_in, b2_own, b2_out, b2_in,
    copy_sem, load_kv, load_q, load_o, q_s, q_down, st_s, st_down, kv_s, dq_s, via_s, g_s, tp_s, a_s, a2_s, b_s, b2_s,
    qd_r, st_r, kv_r, dq_r, via_r, g_r, tp_r, a_r, a2_r, b_r, b2_r,
):
    sp = lax.axis_index("sp")
    tp = lax.axis_index("tp")
    sp_n = tgt_n * src_n
    me_t, me_s = sp // src_n, sp % src_n
    x_s = me_s + 1 - 2 * (me_s % 2)
    y_s, d_s = (me_s + 2) % src_n, (x_s + 2) % src_n
    s_peers = [d_s, x_s, y_s]
    t_peers = [lax.rem(me_t + k, tgt_n) for k in range(1, tgt_n)]
    below, above = me_t, tgt_n - 1 - me_t
    paired = jnp.minimum(below, above)
    longer = jnp.where(above > below, 1, -1)
    inner = paired > 0
    order = []
    for j in range(tgt_n - 1):
        both = me_t + (j // 2 + 1) * (1 if j % 2 == 0 else -1)
        order.append(jnp.where(j < 2 * paired, both, me_t + longer * (j - paired + 1)))
    key_m = tgt_n
    me_o, me_i = me_t, me_s
    o_peers, i_peers = t_peers, s_peers
    tp_peers = [lax.rem(tp + k, tp_n) for k in range(1, tp_n)]
    rows = q_hbm.shape[0]
    heads = q_hbm.shape[1] // HEAD_DIM
    chunks = qd.shape[1]
    src_rows = dk.shape[1]
    stacked = dq_acc.shape[3]
    split = (chunks + 1) // 2
    per_chunk = heads // chunks
    per_key = HEADS // KV_HEADS
    scale = 1.0 / math.sqrt(HEAD_DIM)
    kv_col = pl.multiple_of(tp * heads // per_key * HEAD_DIM, HEAD_DIM)

    def t_dev(t):
        return {"sp": t * src_n + me_s, "tp": tp}

    def s_dev(s):
        return {"sp": me_t * src_n + s, "tp": tp}

    o_dev, i_dev = t_dev, s_dev

    def drain(ref, sem):
        pltpu.make_async_copy(ref, ref, sem).wait()

    def tp_dev(p):
        return {"sp": sp, "tp": p}

    def remote(source, target, sent, recv, device):
        return pltpu.make_async_remote_copy(
            src_ref=source, dst_ref=target, send_sem=sent, recv_sem=recv,
            device_id=device, device_id_type=MESH,
        )

    barrier = pltpu.get_barrier_semaphore()
    def greet(device):
        pl.semaphore_signal(barrier, inc=1, device_id=device, device_id_type=MESH)

    for s in (x_s, y_s):
        greet(s_dev(s))
    for p in tp_peers:
        greet(tp_dev(p))

    @pl.when(above > 0)
    def _():
        greet(t_dev(me_t + 1))

    @pl.when(below > 0)
    def _():
        greet(t_dev(me_t - 1))

    piece = src_rows // HALVES
    chunk_w = per_chunk * HEAD_DIM
    kv_loads = [
        pltpu.make_async_copy(
            ref.at[pl.ds(h * piece, piece), pl.ds(kv_col, HEAD_DIM)],
            kvs.at[me_s, h, i], load_kv,
        )
        for h in range(HALVES) for i, ref in enumerate((key_hbm, value_hbm))
    ]
    q_loads = [
        pltpu.make_async_copy(
            ref.at[:, pl.ds(c * chunk_w, chunk_w)], qd.at[me_t, c, i], load_q.at[c]
        )
        for c in range(chunks) for i, ref in enumerate((q_hbm, d_hbm))
    ]
    loads = [
        pltpu.make_async_copy(o_hbm, o_own, load_o.at[0]),
        pltpu.make_async_copy(lse_hbm, lse_own, load_o.at[1]),
    ]
    late = [pltpu.make_async_copy(source_hbm, src, copy_sem.at[0])]
    for i, ref in enumerate((kw_hbm, vw_hbm)):
        late.append(pltpu.make_async_copy(ref, weights.at[i], copy_sem.at[1 + i]))
    for copy in kv_loads + q_loads + loads:
        copy.start()

    def q_copy(block, t, c, sem):
        return remote(qd.at[block, c], qd.at[block, c], sem, qd_r.at[block, c], t_dev(t))

    def kv_copy(block, s, h):
        return remote(kvs.at[block, h], kvs.at[block, h], kv_s, kv_r.at[block, h], s_dev(s))

    def stat_copy(block, t, sem):
        return remote(stats.at[block], stats.at[block], sem, st_r.at[block], t_dev(t))

    def on_line(act):
        @pl.when(above > 0)
        def _():
            act(me_t + 1, q_s.at[me_t], st_s.at[me_t])

        @pl.when(below > 0)
        def _():
            act(me_t - 1, q_down, st_down)

    sides = jnp.minimum(above, 1) + jnp.minimum(below, 1)
    pl.semaphore_wait(barrier, sides + 1 + tp_n)
    drain(qd.at[me_t, 0], load_q.at[0])
    on_line(lambda t, q, st: q_copy(me_t, t, 0, q).start())
    drain(kvs.at[me_s], load_kv)
    for h in range(HALVES):
        kv_copy(me_s, x_s, HALVES - 1 - h).start()
        kv_copy(me_s, y_s, h).start()
    for c in range(1, chunks):
        drain(qd.at[me_t, c], load_q.at[c])
    for copy in loads:
        copy.wait()
    ones = jnp.ones((8, HEAD_DIM), F32)
    for h in range(heads):
        cols = pl.ds(h * HEAD_DIM, HEAD_DIM)
        c = h // per_chunk
        grad = qd[me_t, c, 1, :, pl.ds(h % per_chunk * HEAD_DIM, HEAD_DIM)]
        prod = grad.astype(F32) * o_own[:, cols].astype(F32)
        delta = dot_nt(ones, prod, lax.Precision.HIGHEST)
        stats[me_t, h : h + 1] = lse_own[h : h + 1, :] * LOG2E
        stats[me_t, heads + h : heads + h + 1] = delta[0:1, :]
    on_line(lambda t, q, st: stat_copy(me_t, t, st).start())
    for c in range(1, chunks):
        on_line(lambda t, q, st, c=c: q_copy(me_t, t, c, q).start())
    for copy in late:
        copy.start()
    dk[...] = jnp.zeros_like(dk)
    dv[...] = jnp.zeros_like(dv)
    dq_acc[...] = jnp.zeros_like(dq_acc)

    def stack(t, i, low, high):
        return jnp.concatenate(
            [
                qd[t, c, i, :, h * HEAD_DIM : (h + 1) * HEAD_DIM]
                for c in range(low, high) for h in range(per_chunk)
            ],
            axis=0,
        )

    def stat(t, i, low, high):
        first = i * heads + low * per_chunk
        count = (high - low) * per_chunk
        return jnp.concatenate([stats[t, first + h : first + h + 1] for h in range(count)], axis=1)

    def keys(s, i):
        return kvs[s, :, i].reshape(src_rows, HEAD_DIM)

    def tile(t, s, low=0, high=chunks):
        if low == high:
            return
        q, d = stack(t, 0, low, high), stack(t, 1, low, high)
        k, v = keys(s, 0), keys(s, 1)
        scores = dot_nt(k, q)
        probs = jnp.exp2(scores * (scale * LOG2E) - stat(t, 0, low, high))
        dprobs = dot_nt(v, d)
        dscores = (probs * (dprobs - stat(t, 1, low, high))).astype(BF16)
        probs = probs.astype(BF16)
        dv[s] += dot_nn(probs, d)
        dk[s] += dot_nn(dscores, q)
        part_q = dot_tn(k, dscores)
        for c in range(low, high):
            span = (c - low) * stacked
            dq_acc[t, c] += part_q[:, span : span + stacked]

    def got_q(j, c):
        q_copy(order[j], me_t, c, q_down).wait_recv()

    def forward(j, act):
        @pl.when(order[j] > me_t)
        def _():
            act(me_t - 1)

        @pl.when(order[j] < me_t)
        def _():
            act(me_t + 1)

    def pass_q(j, c):
        @pl.when(inner)
        def _():
            got_q(j, c)
            forward(j, lambda t: q_copy(order[j], t, c, q_s.at[order[j]]).start())
            if c == split - 1:
                got_stats(order[j])
                forward(j, lambda t: stat_copy(order[j], t, st_s.at[order[j]]).start())

    def last_q(j, c):
        @pl.when(jnp.logical_not(inner))
        def _():
            got_q(j, c)
            if c == split - 1:
                got_stats(order[j])

    def got_stats(t):
        stat_copy(t, me_t, st_down).wait_recv()

    def got_kv(s, h):
        kv_copy(s, s, h).wait_recv()

    def dq_copy(t):
        return remote(dq_out.at[t], dq_in.at[me_t], dq_s, dq_r, t_dev(t))

    def g_part(s, i, h):
        span = pl.ds(h * piece, piece)
        return dv[s, span] if i else dk[s, span] * scale

    def via_copy(i, h):
        return remote(
            d_out.at[i, h], g_via.at[i, h], via_s, via_r.at[i, h], s_dev((x_s, y_s)[h])
        )

    def g_copy(i, n, h):
        return remote(
            g_out.at[i, n, h], g_in.at[i, n, h], g_s, g_r.at[i],
            s_dev((x_s, y_s)[n]),
        )

    def send_via(i):
        for h in range(HALVES):
            d_out[i, h] = g_part(d_s, i, h).astype(BF16)
            via_copy(i, h).start()

    def send_plain(i, n):
        g_out[i, n, n] = g_part((x_s, y_s)[n], i, n).astype(BF16)
        g_copy(i, n, n).start()

    def send_sum(i):
        for h in range(HALVES):
            n = 1 - h
            via_copy(i, h).wait_recv()
            total = g_part((x_s, y_s)[n], i, h) + g_via[i, h].astype(F32)
            g_out[i, n, h] = total.astype(BF16)
            g_copy(i, n, h).start()

    def send_dq(t):
        dq_out[t] = (dq_acc[t] * scale).astype(BF16)
        dq_copy(t).start()

    def edge(t):
        return inner & ((t == 0) | (t == tgt_n - 1))

    def early_dq(t):
        @pl.when(jnp.logical_not(edge(t)))
        def _():
            send_dq(t)

    everyone = [me_s, x_s, y_s, d_s]
    tile(me_t, me_s)
    got_kv(y_s, 0)
    kv_copy(y_s, x_s, 0).start()
    for h in range(1, HALVES):
        got_kv(x_s, h)
        kv_copy(x_s, y_s, h).start()
    for c in range(split):
        pass_q(0, c)
        last_q(0, c)
        pass_q(1, c)
    tile(order[0], me_s, 0, split)
    for h in range(1, HALVES):
        got_kv(y_s, h)
    got_kv(x_s, 0)
    for c in range(split, chunks):
        pass_q(0, c)
        last_q(0, c)
        pass_q(1, c)
    tile(order[0], me_s, split, chunks)
    for s in (x_s, y_s):
        tile(me_t, s)
    tile(order[0], x_s)
    for c in range(split):
        pass_q(2, c)
    for h in range(HALVES):
        got_kv(d_s, h)
    tile(order[0], y_s)
    for t in (me_t, order[0]):
        tile(t, d_s)
    early_dq(order[0])
    for c in range(split, chunks):
        pass_q(2, c)
    for c in range(chunks):
        last_q(1, c)
    for s in everyone:
        tile(order[1], s)
    early_dq(order[1])
    for j in range(2, tgt_n - 1):
        for c in range(chunks):
            if j > 2:
                pass_q(j, c)
            last_q(j, c)
            if c == split - 1:
                for s in everyone:
                    tile(order[j], s, 0, split)
        if j < tgt_n - 2:
            for s in everyone:
                tile(order[j], s, split, chunks)
            early_dq(order[j])
    for n, s in enumerate([d_s, x_s, y_s, me_s]):
        tile(order[-1], s, split, chunks)
        if n == 0:
            send_via(0)
        elif n < 3:
            send_plain(0, n - 1)
    send_dq(order[-1])
    for t in order[:-1]:
        @pl.when(edge(t))
        def _(t=t):
            send_dq(t)

    send_sum(0)
    send_via(1)
    for n in range(2):
        send_plain(1, n)

    def reduce_g(i):
        drain(g_in.at[i], g_r.at[i])
        for h in range(HALVES):
            total = g_part(me_s, i, h)
            for n in range(2):
                total += g_in[i, n, h].astype(F32)
            tp_own[i, h * piece : (h + 1) * piece] = total.astype(BF16)
        for p in tp_peers:
            remote(
                tp_own.at[i], tp_in.at[tp, i], tp_s, tp_r.at[i], tp_dev(p)
            ).start()
        tp_in[tp, i] = tp_own[i]

    def gather_g(i):
        drain(tp_in.at[0 : tp_n - 1, i], tp_r.at[i])
        for g in range(KV_HEADS):
            owners = [p for p in range(tp_n) if p * heads // per_key == g]
            half = tp_in[owners[0], i]
            if len(owners) > 1:
                total = half.astype(F32)
                for p in owners[1:]:
                    total += tp_in[p, i].astype(F32)
                half = total.astype(BF16)
            kv_ref[:, pl.ds((i * KV_HEADS + g) * HEAD_DIM, HEAD_DIM)] = half

    reduce_g(0)
    late[0].wait()
    gather_g(0)
    pieces, part, cut = a2_own.shape[0], a2_own.shape[2], a2_own.shape[3]
    key_half = kv_ref[:, 0 : KV_HEADS * HEAD_DIM]
    w_scale = 1.0 / math.sqrt(src_total)

    def a_copy(p, i):
        return remote(
            a_out.at[p, i], a_in.at[p, me_i], a_s, a_r.at[p], i_dev(i)
        )

    def a2_copy(p, o):
        return remote(
            a2_out.at[p, o], a2_in.at[p, me_o], a2_s, a2_r, o_dev(o)
        )

    def a_part(p):
        partial = dot_tn(key_half, src[:, p * cut : (p + 1) * cut]) * w_scale
        for o in range(key_m):
            for i in range(key_n):
                low = (o * key_n + i) * part
                a_out[p, i, o] = partial[low : low + part].astype(BF16)
        for i in i_peers:
            a_copy(p, i).start()

    a_part(0)
    partial = dot_tn(key_half, src[:, pieces * cut :]) * w_scale
    for o in range(key_m):
        for i in range(key_n):
            low = (o * key_n + i) * part
            b_out[o, i] = partial[low : low + part].astype(BF16)
    for o in o_peers:
        remote(b_out.at[o], b_in.at[me_o], b_s, b_r, o_dev(o)).start()
    for p in range(1, pieces):
        a_part(p)
    send_sum(1)

    def add_source(i):
        width = KV_HEADS * HEAD_DIM
        span = sg_ref.shape[1] // 4

        def body(n, carry):
            cols = pl.ds(pl.multiple_of(n * span, HEAD_DIM), span)
            term = dot_nt(kv_ref[:, i * width : (i + 1) * width], weights[i, cols, :])
            sg_ref[:, cols] = sg_ref[:, cols] + term if i else term
            return carry

        lax.fori_loop(0, 4, body, 0)

    def a_sum(p):
        total = a_out[p, me_i].astype(F32)
        drain(a_in.at[p, 0 : key_n - 1], a_r.at[p])
        for i in i_peers:
            total += a_in[p, i].astype(F32)
        a2_own[p] = total
        a2_out[p] = total.astype(BF16)
        for o in o_peers:
            a2_copy(p, o).start()

    for copy in late[1:]:
        copy.wait()
    add_source(0)
    a_sum(0)
    total = b_out[me_o].astype(F32)
    drain(b_in.at[0 : key_m - 1], b_r)
    for o in o_peers:
        total += b_in[o].astype(F32)
    b2_own[...] = total
    b2_out[...] = total.astype(BF16)
    for i in i_peers:
        remote(b2_out.at[i], b2_in.at[me_i], b2_s, b2_r, i_dev(i)).start()
    for p in range(1, pieces):
        a_sum(p)

    reduce_g(1)
    gather_g(1)
    add_source(1)
    dq_total = dq_acc[me_t] * scale
    drain(dq_in.at[0 : tgt_n - 1], dq_r)
    for t in t_peers:
        dq_total += dq_in[t].astype(F32)
    for h in range(heads):
        low = h % per_chunk * rows
        block = dq_total[h // per_chunk, :, low : low + rows]
        dq_ref[:, h * HEAD_DIM : (h + 1) * HEAD_DIM] = block.T

    def done_line(t, q, st):
        drain(qd.at[me_t], q)
        drain(stats.at[me_t], st)

    on_line(done_line)

    @pl.when(inner)
    def _():
        for t in order:
            drain(qd.at[t], q_s.at[t])
            drain(stats.at[t], st_s.at[t])

    drain(kvs.at[0 : src_n - 1], kv_s)
    drain(dq_out.at[0 : tgt_n - 1], dq_s)
    drain(d_out, via_s)
    drain(g_out, g_s)
    drain(tp_in.at[0 : tp_n - 1], tp_s)
    drain(a_out.at[:, 0 : key_n - 1], a_s)
    drain(a2_out.at[:, 0 : key_m - 1], a2_s)
    drain(b_out.at[0 : key_m - 1], b_s)
    drain(b2_out.at[0 : key_n - 1], b2_s)

    total = b2_own[me_i]
    drain(b2_in.at[0 : key_n - 1], b2_r)
    for i in i_peers:
        total += b2_in[i].astype(F32)
    kg_ref[:, pieces * cut :] = total
    drain(a2_in.at[:, 0 : key_m - 1], a2_r)
    for p in range(pieces):
        total = a2_own[p, me_o]
        for o in o_peers:
            total += a2_in[p, o].astype(F32)
        kg_ref[:, p * cut : (p + 1) * cut] = total


def finish(*refs):
    *refs, sem = refs
    copies = [
        pltpu.make_async_copy(value, out, sem.at[n])
        for n, (value, out) in enumerate(zip(refs[:3], refs[3:]))
    ]
    for copy in copies:
        copy.start()
    for copy in copies:
        copy.wait()


def shards(
    tgt_n, src_n, tp_n,
    queries, attn_out, out_grad, row_lse, source, saved_keys, saved_values, key_weight, value_weight
):
    heads = row_lse.shape[1]
    rows, width = queries.shape
    src_rows, columns = source.shape
    kv_width = KV_HEADS * HEAD_DIM
    sp_n = tgt_n * src_n
    part = kv_width // sp_n
    key_n, key_m = src_n, tgt_n
    chunks = math.gcd(heads, 2)
    stacked = heads // chunks * rows
    cut = columns // (PIECES + 1) // HEAD_DIM * HEAD_DIM
    rest = columns - PIECES * cut
    dma = pltpu.SemaphoreType.DMA
    vmem = pl.BlockSpec(memory_space=pltpu.VMEM)
    hbm = pl.BlockSpec(memory_space=pltpu.HBM)
    scratch = [
        pltpu.VMEM((src_rows, 2 * kv_width), BF16),
        pltpu.VMEM((2, columns, kv_width), BF16),
        pltpu.VMEM((rows, width), BF16),
        pltpu.VMEM((heads, rows), F32),
        pltpu.VMEM((tgt_n, chunks, 2, rows, width // chunks), BF16),
        pltpu.VMEM((tgt_n, 2 * heads, rows), F32),
        pltpu.VMEM((src_n, HALVES, 2, src_rows // HALVES, HEAD_DIM), BF16),
        pltpu.VMEM((src_n, src_rows, HEAD_DIM), F32),
        pltpu.VMEM((src_n, src_rows, HEAD_DIM), F32),
        pltpu.VMEM((tgt_n, chunks, HEAD_DIM, stacked), F32),
        pltpu.VMEM((tgt_n, chunks, HEAD_DIM, stacked), BF16),
        pltpu.VMEM((tgt_n, chunks, HEAD_DIM, stacked), BF16),
        pltpu.VMEM((2, HALVES, src_rows // HALVES, HEAD_DIM), BF16),
        pltpu.VMEM((2, HALVES, src_rows // HALVES, HEAD_DIM), BF16),
        pltpu.VMEM((2, 2, HALVES, src_rows // HALVES, HEAD_DIM), BF16),
        pltpu.VMEM((2, 2, HALVES, src_rows // HALVES, HEAD_DIM), BF16),
        pltpu.VMEM((2, src_rows, HEAD_DIM), BF16),
        pltpu.VMEM((tp_n, 2, src_rows, HEAD_DIM), BF16),
        pltpu.VMEM((src_rows, columns), BF16),
        pltpu.VMEM((PIECES, key_n, key_m, part, cut), BF16),
        pltpu.VMEM((PIECES, key_n, key_m, part, cut), BF16),
        pltpu.VMEM((PIECES, key_m, part, cut), F32),
        pltpu.VMEM((PIECES, key_m, part, cut), BF16),
        pltpu.VMEM((PIECES, key_m, part, cut), BF16),
        pltpu.VMEM((key_m, key_n, part, rest), BF16),
        pltpu.VMEM((key_m, key_n, part, rest), BF16),
        pltpu.VMEM((key_n, part, rest), F32),
        pltpu.VMEM((key_n, part, rest), BF16),
        pltpu.VMEM((key_n, part, rest), BF16),
        dma((3,)),
        dma(()),
        dma((chunks,)),
        dma((2,)),
    ]
    for shape in (
        (tgt_n,), (), (tgt_n,), (), (), (), (), (), (), (), (), (), (),
        (tgt_n, chunks), (tgt_n,), (src_n, HALVES), (), (2, HALVES), (2,), (2,), (PIECES,),
        (), (), (),
    ):
        scratch.append(dma(shape))
    shapes = ((rows, width), (src_rows, columns), (part, columns))
    grads = pl.pallas_call(
        functools.partial(kernel, tgt_n, src_n, key_n, tp_n, src_rows * sp_n),
        out_shape=[pltpu.VMEM(shape, F32) for shape in shapes],
        in_specs=[hbm] * 9,
        out_specs=[vmem] * 3,
        scratch_shapes=scratch,
        compiler_params=pltpu.CompilerParams(
            collective_id=0, has_side_effects=True,
            vmem_limit_bytes=VMEM_BYTES - 4 * sum(map(math.prod, shapes)),
        ),
        name="attention_grads",
    )(
        queries, attn_out, out_grad, row_lse.T, saved_keys, saved_values, source,
        key_weight, value_weight,
    )
    return tuple(pl.pallas_call(
        finish,
        out_shape=[jax.ShapeDtypeStruct(shape, F32) for shape in shapes],
        in_specs=[vmem] * 3,
        out_specs=[hbm] * 3,
        scratch_shapes=[dma((3,))],
        compiler_params=pltpu.CompilerParams(vmem_limit_bytes=2**20),
        name="write_grads",
    )(*grads))


def solution(mesh):
    sp_n, tp_n = mesh.shape["sp"], mesh.shape["tp"]
    src_n = math.gcd(sp_n, 4)
    in_specs = (
        P("sp", "tp"),
        P("sp", "tp"),
        P("sp", "tp"),
        P("sp", "tp"),
        P("sp", "tp"),
        P("sp", None),
        P("sp", None),
        P("tp", None),
        P("tp", None),
    )
    out_specs = (P("sp", "tp"), P("sp", "tp"), P("sp", "tp"))
    return jax.shard_map(
        functools.partial(shards, sp_n // src_n, src_n, tp_n),
        mesh=mesh, in_specs=in_specs, out_specs=out_specs, check_vma=False,
    )
```

```python
import functools
import math

import jax
import jax.numpy as jnp
from jax import lax
from jax.experimental import pallas as pl
from jax.experimental.pallas import tpu as pltpu
from jax.sharding import PartitionSpec as P

HEADS = 8
KV_HEADS = 2
HEAD_DIM = 128
HALVES = 2
PIECES = 3
LOG2E = 1.0 / math.log(2.0)
MESH = pl.DeviceIdType.MESH
F32 = jnp.float32
BF16 = jnp.bfloat16
VMEM_BYTES = 67_043_328


def dot_nt(left, right, precision=None):
    return lax.dot_general(
        left, right, (((1,), (1,)), ((), ())), preferred_element_type=F32, precision=precision
    )


def dot_tn(left, right):
    return lax.dot_general(left, right, (((0,), (0,)), ((), ())), preferred_element_type=F32)


def dot_nn(left, right):
    return jnp.dot(left, right, preferred_element_type=F32)


def kernel(
    tgt_n, src_n, key_n, tp_n, src_total,
    q_hbm, o_hbm, d_hbm, lse_hbm, key_hbm, value_hbm, source_hbm, kw_hbm, vw_hbm,
    dq_ref, sg_ref, kg_ref,
    kv_ref, weights,    o_own, lse_own, qd, stats, kvs, dk, dv, dq_acc, dq_out, dq_in, d_out, g_via, g_out, g_in, tp_own, tp_in,
    src, a_out, a_in, a2_own, a2_out, a2_in, b_out, b_in, b2_own, b2_out, b2_in,
    copy_sem, load_kv, load_q, load_o, q_s, q_down, st_s, st_down, kv_s, dq_s, via_s, g_s, tp_s, a_s, a2_s, b_s, b2_s,
    qd_r, st_r, kv_r, dq_r, via_r, g_r, tp_r, a_r, a2_r, b_r, b2_r,
):
    sp = lax.axis_index("sp")
    tp = lax.axis_index("tp")
    sp_n = tgt_n * src_n
    me_t, me_s = sp // src_n, sp % src_n
    x_s = me_s + 1 - 2 * (me_s % 2)
    y_s, d_s = (me_s + 2) % src_n, (x_s + 2) % src_n
    s_peers = [d_s, x_s, y_s]
    t_peers = [lax.rem(me_t + k, tgt_n) for k in range(1, tgt_n)]
    below, above = me_t, tgt_n - 1 - me_t
    paired = jnp.minimum(below, above)
    longer = jnp.where(above > below, 1, -1)
    inner = paired > 0
    order = []
    for j in range(tgt_n - 1):
        both = me_t + (j // 2 + 1) * (1 if j % 2 == 0 else -1)
        order.append(jnp.where(j < 2 * paired, both, me_t + longer * (j - paired + 1)))
    key_m = tgt_n
    me_o, me_i = me_t, me_s
    o_peers, i_peers = t_peers, s_peers
    tp_peers = [lax.rem(tp + k, tp_n) for k in range(1, tp_n)]
    rows = q_hbm.shape[0]
    heads = q_hbm.shape[1] // HEAD_DIM
    chunks = qd.shape[1]
    src_rows = dk.shape[1]
    stacked = dq_acc.shape[3]
    split = (chunks + 1) // 2
    per_chunk = heads // chunks
    per_key = HEADS // KV_HEADS
    scale = 1.0 / math.sqrt(HEAD_DIM)
    kv_col = pl.multiple_of(tp * heads // per_key * HEAD_DIM, HEAD_DIM)

    def t_dev(t):
        return {"sp": t * src_n + me_s, "tp": tp}

    def s_dev(s):
        return {"sp": me_t * src_n + s, "tp": tp}

    o_dev, i_dev = t_dev, s_dev

    def drain(ref, sem):
        pltpu.make_async_copy(ref, ref, sem).wait()

    def tp_dev(p):
        return {"sp": sp, "tp": p}

    def remote(source, target, sent, recv, device):
        return pltpu.make_async_remote_copy(
            src_ref=source, dst_ref=target, send_sem=sent, recv_sem=recv,
            device_id=device, device_id_type=MESH,
        )

    barrier = pltpu.get_barrier_semaphore()
    def greet(device):
        pl.semaphore_signal(barrier, inc=1, device_id=device, device_id_type=MESH)

    for s in (x_s, y_s):
        greet(s_dev(s))
    for p in tp_peers:
        greet(tp_dev(p))

    @pl.when(above > 0)
    def _():
        greet(t_dev(me_t + 1))

    @pl.when(below > 0)
    def _():
        greet(t_dev(me_t - 1))

    piece = src_rows // HALVES
    chunk_w = per_chunk * HEAD_DIM
    kv_loads = [
        pltpu.make_async_copy(
            ref.at[pl.ds(h * piece, piece), pl.ds(kv_col, HEAD_DIM)],
            kvs.at[me_s, h, i], load_kv,
        )
        for h in range(HALVES) for i, ref in enumerate((key_hbm, value_hbm))
    ]
    q_loads = [
        pltpu.make_async_copy(
            ref.at[:, pl.ds(c * chunk_w, chunk_w)], qd.at[me_t, c, i], load_q.at[c]
        )
        for c in range(chunks) for i, ref in enumerate((q_hbm, d_hbm))
    ]
    loads = [
        pltpu.make_async_copy(o_hbm, o_own, load_o.at[0]),
        pltpu.make_async_copy(lse_hbm, lse_own, load_o.at[1]),
    ]
    late = [pltpu.make_async_copy(source_hbm, src, copy_sem.at[0])]
    for i, ref in enumerate((kw_hbm, vw_hbm)):
        late.append(pltpu.make_async_copy(ref, weights.at[i], copy_sem.at[1 + i]))
    for copy in kv_loads + q_loads + loads:
        copy.start()

    def q_copy(block, t, c, sem):
        return remote(qd.at[block, c], qd.at[block, c], sem, qd_r.at[block, c], t_dev(t))

    def kv_copy(block, s, h):
        return remote(kvs.at[block, h], kvs.at[block, h], kv_s, kv_r.at[block, h], s_dev(s))

    def stat_copy(block, t, sem):
        return remote(stats.at[block], stats.at[block], sem, st_r.at[block], t_dev(t))

    def on_line(act):
        @pl.when(above > 0)
        def _():
            act(me_t + 1, q_s.at[me_t], st_s.at[me_t])

        @pl.when(below > 0)
        def _():
            act(me_t - 1, q_down, st_down)

    sides = jnp.minimum(above, 1) + jnp.minimum(below, 1)
    pl.semaphore_wait(barrier, sides + 1 + tp_n)
    drain(qd.at[me_t, 0], load_q.at[0])
    on_line(lambda t, q, st: q_copy(me_t, t, 0, q).start())
    drain(kvs.at[me_s], load_kv)
    for h in range(HALVES):
        kv_copy(me_s, x_s, HALVES - 1 - h).start()
        kv_copy(me_s, y_s, h).start()
    for c in range(1, chunks):
        drain(qd.at[me_t, c], load_q.at[c])
    for copy in loads:
        copy.wait()
    ones = jnp.ones((8, HEAD_DIM), F32)
    for h in range(heads):
        cols = pl.ds(h * HEAD_DIM, HEAD_DIM)
        c = h // per_chunk
        grad = qd[me_t, c, 1, :, pl.ds(h % per_chunk * HEAD_DIM, HEAD_DIM)]
        prod = grad.astype(F32) * o_own[:, cols].astype(F32)
        delta = dot_nt(ones, prod, lax.Precision.HIGHEST)
        stats[me_t, h : h + 1] = lse_own[h : h + 1, :] * LOG2E
        stats[me_t, heads + h : heads + h + 1] = delta[0:1, :]
    on_line(lambda t, q, st: stat_copy(me_t, t, st).start())
    for c in range(1, chunks):
        on_line(lambda t, q, st, c=c: q_copy(me_t, t, c, q).start())
    for copy in late:
        copy.start()
    dk[...] = jnp.zeros_like(dk)
    dv[...] = jnp.zeros_like(dv)
    dq_acc[...] = jnp.zeros_like(dq_acc)

    def stack(t, i, low, high):
        return jnp.concatenate(
            [
                qd[t, c, i, :, h * HEAD_DIM : (h + 1) * HEAD_DIM]
                for c in range(low, high) for h in range(per_chunk)
            ],
            axis=0,
        )

    def stat(t, i, low, high):
        first = i * heads + low * per_chunk
        count = (high - low) * per_chunk
        return jnp.concatenate([stats[t, first + h : first + h + 1] for h in range(count)], axis=1)

    def keys(s, i):
        return kvs[s, :, i].reshape(src_rows, HEAD_DIM)

    def tile(t, s, low=0, high=chunks):
        if low == high:
            return
        q, d = stack(t, 0, low, high), stack(t, 1, low, high)
        k, v = keys(s, 0), keys(s, 1)
        scores = dot_nt(k, q)
        probs = jnp.exp2(scores * (scale * LOG2E) - stat(t, 0, low, high))
        dprobs = dot_nt(v, d)
        dscores = (probs * (dprobs - stat(t, 1, low, high))).astype(BF16)
        probs = probs.astype(BF16)
        dv[s] += dot_nn(probs, d)
        dk[s] += dot_nn(dscores, q)
        part_q = dot_tn(k, dscores)
        for c in range(low, high):
            span = (c - low) * stacked
            dq_acc[t, c] += part_q[:, span : span + stacked]

    def got_q(j, c):
        q_copy(order[j], me_t, c, q_down).wait_recv()

    def forward(j, act):
        @pl.when(order[j] > me_t)
        def _():
            act(me_t - 1)

        @pl.when(order[j] < me_t)
        def _():
            act(me_t + 1)

    def pass_q(j, c):
        @pl.when(inner)
        def _():
            got_q(j, c)
            forward(j, lambda t: q_copy(order[j], t, c, q_s.at[order[j]]).start())
            if c == split - 1:
                got_stats(order[j])
                forward(j, lambda t: stat_copy(order[j], t, st_s.at[order[j]]).start())

    def last_q(j, c):
        @pl.when(jnp.logical_not(inner))
        def _():
            got_q(j, c)
            if c == split - 1:
                got_stats(order[j])

    def got_stats(t):
        stat_copy(t, me_t, st_down).wait_recv()

    def got_kv(s, h):
        kv_copy(s, s, h).wait_recv()

    def dq_copy(t):
        return remote(dq_out.at[t], dq_in.at[me_t], dq_s, dq_r, t_dev(t))

    def g_part(s, i, h):
        span = pl.ds(h * piece, piece)
        return dv[s, span] if i else dk[s, span] * scale

    def via_copy(i, h):
        return remote(
            d_out.at[i, h], g_via.at[i, h], via_s, via_r.at[i, h], s_dev((x_s, y_s)[h])
        )

    def g_copy(i, n, h):
        return remote(
            g_out.at[i, n, h], g_in.at[i, n, h], g_s, g_r.at[i],
            s_dev((x_s, y_s)[n]),
        )

    def send_via(i):
        for h in range(HALVES):
            d_out[i, h] = g_part(d_s, i, h).astype(BF16)
            via_copy(i, h).start()

    def send_plain(i, n):
        g_out[i, n, n] = g_part((x_s, y_s)[n], i, n).astype(BF16)
        g_copy(i, n, n).start()

    def send_sum(i):
        for h in range(HALVES):
            n = 1 - h
            via_copy(i, h).wait_recv()
            total = g_part((x_s, y_s)[n], i, h) + g_via[i, h].astype(F32)
            g_out[i, n, h] = total.astype(BF16)
            g_copy(i, n, h).start()

    def send_dq(t):
        dq_out[t] = (dq_acc[t] * scale).astype(BF16)
        dq_copy(t).start()

    def edge(t):
        return inner & ((t == 0) | (t == tgt_n - 1))

    def early_dq(t):
        @pl.when(jnp.logical_not(edge(t)))
        def _():
            send_dq(t)

    everyone = [me_s, x_s, y_s, d_s]
    tile(me_t, me_s)
    got_kv(y_s, 0)
    kv_copy(y_s, x_s, 0).start()
    for h in range(1, HALVES):
        got_kv(x_s, h)
        kv_copy(x_s, y_s, h).start()
    for c in range(split):
        pass_q(0, c)
        last_q(0, c)
        pass_q(1, c)
    tile(order[0], me_s, 0, split)
    for h in range(1, HALVES):
        got_kv(y_s, h)
    got_kv(x_s, 0)
    for c in range(split, chunks):
        pass_q(0, c)
        last_q(0, c)
        pass_q(1, c)
    tile(order[0], me_s, split, chunks)
    for s in (x_s, y_s):
        tile(me_t, s)
    tile(order[0], x_s)
    for c in range(split):
        pass_q(2, c)
    for h in range(HALVES):
        got_kv(d_s, h)
    tile(order[0], y_s)
    for t in (me_t, order[0]):
        tile(t, d_s)
    early_dq(order[0])
    for c in range(split, chunks):
        pass_q(2, c)
    for low, high in ((0, split), (split, chunks)):
        for c in range(low, high):
            last_q(1, c)
        for s in everyone:
            tile(order[1], s, low, high)
    early_dq(order[1])
    for j in range(2, tgt_n - 1):
        for c in range(chunks):
            if j > 2:
                pass_q(j, c)
            last_q(j, c)
            if c == split - 1:
                for s in everyone:
                    tile(order[j], s, 0, split)
        if j < tgt_n - 2:
            for s in everyone:
                tile(order[j], s, split, chunks)
            early_dq(order[j])
    for n, s in enumerate([d_s, x_s, y_s, me_s]):
        tile(order[-1], s, split, chunks)
        if n == 0:
            send_via(0)
        elif n < 3:
            send_plain(0, n - 1)
    send_dq(order[-1])
    for t in order[:-1]:
        @pl.when(edge(t))
        def _(t=t):
            send_dq(t)

    send_sum(0)
    send_via(1)
    for n in range(2):
        send_plain(1, n)

    def reduce_g(i):
        drain(g_in.at[i], g_r.at[i])
        for h in range(HALVES):
            total = g_part(me_s, i, h)
            for n in range(2):
                total += g_in[i, n, h].astype(F32)
            tp_own[i, h * piece : (h + 1) * piece] = total.astype(BF16)
        for p in tp_peers:
            remote(
                tp_own.at[i], tp_in.at[tp, i], tp_s, tp_r.at[i], tp_dev(p)
            ).start()
        tp_in[tp, i] = tp_own[i]

    def gather_g(i):
        drain(tp_in.at[0 : tp_n - 1, i], tp_r.at[i])
        for g in range(KV_HEADS):
            owners = [p for p in range(tp_n) if p * heads // per_key == g]
            half = tp_in[owners[0], i]
            if len(owners) > 1:
                total = half.astype(F32)
                for p in owners[1:]:
                    total += tp_in[p, i].astype(F32)
                half = total.astype(BF16)
            kv_ref[:, pl.ds((i * KV_HEADS + g) * HEAD_DIM, HEAD_DIM)] = half

    reduce_g(0)
    late[0].wait()
    gather_g(0)
    pieces, part, cut = a2_own.shape[0], a2_own.shape[2], a2_own.shape[3]
    key_half = kv_ref[:, 0 : KV_HEADS * HEAD_DIM]
    w_scale = 1.0 / math.sqrt(src_total)

    def a_copy(p, i):
        return remote(
            a_out.at[p, i], a_in.at[p, me_i], a_s, a_r.at[p], i_dev(i)
        )

    def a2_copy(p, o):
        return remote(
            a2_out.at[p, o], a2_in.at[p, me_o], a2_s, a2_r, o_dev(o)
        )

    def a_part(p):
        partial = dot_tn(key_half, src[:, p * cut : (p + 1) * cut]) * w_scale
        for o in range(key_m):
            for i in range(key_n):
                low = (o * key_n + i) * part
                a_out[p, i, o] = partial[low : low + part].astype(BF16)
        for i in i_peers:
            a_copy(p, i).start()

    a_part(0)
    partial = dot_tn(key_half, src[:, pieces * cut :]) * w_scale
    for o in range(key_m):
        for i in range(key_n):
            low = (o * key_n + i) * part
            b_out[o, i] = partial[low : low + part].astype(BF16)
    for o in o_peers:
        remote(b_out.at[o], b_in.at[me_o], b_s, b_r, o_dev(o)).start()
    for p in range(1, pieces):
        a_part(p)
    send_sum(1)

    def add_source(i):
        width = KV_HEADS * HEAD_DIM
        span = sg_ref.shape[1] // 4

        def body(n, carry):
            cols = pl.ds(pl.multiple_of(n * span, HEAD_DIM), span)
            term = dot_nt(kv_ref[:, i * width : (i + 1) * width], weights[i, cols, :])
            sg_ref[:, cols] = sg_ref[:, cols] + term if i else term
            return carry

        lax.fori_loop(0, 4, body, 0)

    def a_sum(p):
        total = a_out[p, me_i].astype(F32)
        drain(a_in.at[p, 0 : key_n - 1], a_r.at[p])
        for i in i_peers:
            total += a_in[p, i].astype(F32)
        a2_own[p] = total
        a2_out[p] = total.astype(BF16)
        for o in o_peers:
            a2_copy(p, o).start()

    for copy in late[1:]:
        copy.wait()
    add_source(0)
    a_sum(0)
    total = b_out[me_o].astype(F32)
    drain(b_in.at[0 : key_m - 1], b_r)
    for o in o_peers:
        total += b_in[o].astype(F32)
    b2_own[...] = total
    b2_out[...] = total.astype(BF16)
    for i in i_peers:
        remote(b2_out.at[i], b2_in.at[me_i], b2_s, b2_r, i_dev(i)).start()
    for p in range(1, pieces):
        a_sum(p)

    reduce_g(1)
    gather_g(1)
    add_source(1)
    dq_total = dq_acc[me_t] * scale
    drain(dq_in.at[0 : tgt_n - 1], dq_r)
    for t in t_peers:
        dq_total += dq_in[t].astype(F32)
    for h in range(heads):
        low = h % per_chunk * rows
        block = dq_total[h // per_chunk, :, low : low + rows]
        dq_ref[:, h * HEAD_DIM : (h + 1) * HEAD_DIM] = block.T

    def done_line(t, q, st):
        drain(qd.at[me_t], q)
        drain(stats.at[me_t], st)

    on_line(done_line)

    @pl.when(inner)
    def _():
        for t in order:
            drain(qd.at[t], q_s.at[t])
            drain(stats.at[t], st_s.at[t])

    drain(kvs.at[0 : src_n - 1], kv_s)
    drain(dq_out.at[0 : tgt_n - 1], dq_s)
    drain(d_out, via_s)
    drain(g_out, g_s)
    drain(tp_in.at[0 : tp_n - 1], tp_s)
    drain(a_out.at[:, 0 : key_n - 1], a_s)
    drain(a2_out.at[:, 0 : key_m - 1], a2_s)
    drain(b_out.at[0 : key_m - 1], b_s)
    drain(b2_out.at[0 : key_n - 1], b2_s)

    total = b2_own[me_i]
    drain(b2_in.at[0 : key_n - 1], b2_r)
    for i in i_peers:
        total += b2_in[i].astype(F32)
    kg_ref[:, pieces * cut :] = total
    drain(a2_in.at[:, 0 : key_m - 1], a2_r)
    for p in range(pieces):
        total = a2_own[p, me_o]
        for o in o_peers:
            total += a2_in[p, o].astype(F32)
        kg_ref[:, p * cut : (p + 1) * cut] = total


def finish(*refs):
    *refs, sem = refs
    copies = [
        pltpu.make_async_copy(value, out, sem.at[n])
        for n, (value, out) in enumerate(zip(refs[:3], refs[3:]))
    ]
    for copy in copies:
        copy.start()
    for copy in copies:
        copy.wait()


def shards(
    tgt_n, src_n, tp_n,
    queries, attn_out, out_grad, row_lse, source, saved_keys, saved_values, key_weight, value_weight
):
    heads = row_lse.shape[1]
    rows, width = queries.shape
    src_rows, columns = source.shape
    kv_width = KV_HEADS * HEAD_DIM
    sp_n = tgt_n * src_n
    part = kv_width // sp_n
    key_n, key_m = src_n, tgt_n
    chunks = math.gcd(heads, 2)
    stacked = heads // chunks * rows
    cut = columns // (PIECES + 1) // HEAD_DIM * HEAD_DIM
    rest = columns - PIECES * cut
    dma = pltpu.SemaphoreType.DMA
    vmem = pl.BlockSpec(memory_space=pltpu.VMEM)
    hbm = pl.BlockSpec(memory_space=pltpu.HBM)
    scratch = [
        pltpu.VMEM((src_rows, 2 * kv_width), BF16),
        pltpu.VMEM((2, columns, kv_width), BF16),
        pltpu.VMEM((rows, width), BF16),
        pltpu.VMEM((heads, rows), F32),
        pltpu.VMEM((tgt_n, chunks, 2, rows, width // chunks), BF16),
        pltpu.VMEM((tgt_n, 2 * heads, rows), F32),
        pltpu.VMEM((src_n, HALVES, 2, src_rows // HALVES, HEAD_DIM), BF16),
        pltpu.VMEM((src_n, src_rows, HEAD_DIM), F32),
        pltpu.VMEM((src_n, src_rows, HEAD_DIM), F32),
        pltpu.VMEM((tgt_n, chunks, HEAD_DIM, stacked), F32),
        pltpu.VMEM((tgt_n, chunks, HEAD_DIM, stacked), BF16),
        pltpu.VMEM((tgt_n, chunks, HEAD_DIM, stacked), BF16),
        pltpu.VMEM((2, HALVES, src_rows // HALVES, HEAD_DIM), BF16),
        pltpu.VMEM((2, HALVES, src_rows // HALVES, HEAD_DIM), BF16),
        pltpu.VMEM((2, 2, HALVES, src_rows // HALVES, HEAD_DIM), BF16),
        pltpu.VMEM((2, 2, HALVES, src_rows // HALVES, HEAD_DIM), BF16),
        pltpu.VMEM((2, src_rows, HEAD_DIM), BF16),
        pltpu.VMEM((tp_n, 2, src_rows, HEAD_DIM), BF16),
        pltpu.VMEM((src_rows, columns), BF16),
        pltpu.VMEM((PIECES, key_n, key_m, part, cut), BF16),
        pltpu.VMEM((PIECES, key_n, key_m, part, cut), BF16),
        pltpu.VMEM((PIECES, key_m, part, cut), F32),
        pltpu.VMEM((PIECES, key_m, part, cut), BF16),
        pltpu.VMEM((PIECES, key_m, part, cut), BF16),
        pltpu.VMEM((key_m, key_n, part, rest), BF16),
        pltpu.VMEM((key_m, key_n, part, rest), BF16),
        pltpu.VMEM((key_n, part, rest), F32),
        pltpu.VMEM((key_n, part, rest), BF16),
        pltpu.VMEM((key_n, part, rest), BF16),
        dma((3,)),
        dma(()),
        dma((chunks,)),
        dma((2,)),
    ]
    for shape in (
        (tgt_n,), (), (tgt_n,), (), (), (), (), (), (), (), (), (), (),
        (tgt_n, chunks), (tgt_n,), (src_n, HALVES), (), (2, HALVES), (2,), (2,), (PIECES,),
        (), (), (),
    ):
        scratch.append(dma(shape))
    shapes = ((rows, width), (src_rows, columns), (part, columns))
    grads = pl.pallas_call(
        functools.partial(kernel, tgt_n, src_n, key_n, tp_n, src_rows * sp_n),
        out_shape=[pltpu.VMEM(shape, F32) for shape in shapes],
        in_specs=[hbm] * 9,
        out_specs=[vmem] * 3,
        scratch_shapes=scratch,
        compiler_params=pltpu.CompilerParams(
            collective_id=0, has_side_effects=True,
            vmem_limit_bytes=VMEM_BYTES - 4 * sum(map(math.prod, shapes)),
        ),
        name="attention_grads",
    )(
        queries, attn_out, out_grad, row_lse.T, saved_keys, saved_values, source,
        key_weight, value_weight,
    )
    return tuple(pl.pallas_call(
        finish,
        out_shape=[jax.ShapeDtypeStruct(shape, F32) for shape in shapes],
        in_specs=[vmem] * 3,
        out_specs=[hbm] * 3,
        scratch_shapes=[dma((3,))],
        compiler_params=pltpu.CompilerParams(vmem_limit_bytes=2**20),
        name="write_grads",
    )(*grads))


def solution(mesh):
    sp_n, tp_n = mesh.shape["sp"], mesh.shape["tp"]
    src_n = math.gcd(sp_n, 4)
    in_specs = (
        P("sp", "tp"),
        P("sp", "tp"),
        P("sp", "tp"),
        P("sp", "tp"),
        P("sp", "tp"),
        P("sp", None),
        P("sp", None),
        P("tp", None),
        P("tp", None),
    )
    out_specs = (P("sp", "tp"), P("sp", "tp"), P("sp", "tp"))
    return jax.shard_map(
        functools.partial(shards, sp_n // src_n, src_n, tp_n),
        mesh=mesh, in_specs=in_specs, out_specs=out_specs, check_vma=False,
    )
```
